256 devices in a mesh: sp: 16 (over y, x), tp: 16 (over z, core).
Axes of the slice: x: 4, y: 4, z: 8, core: 2. Of those that a mesh axis runs over, the one named last changes fastest.
Arguments:
- moe_input: bfloat16 [2048, 2048], P('sp'), may hold values from -6 to 6
- cotangent: bfloat16 [2048, 2048], P('sp'), may hold values from -6 to 6
- route_expert: int32 [2048, 2], P('sp'), may hold values from 0 to 15, all different within a row; in each aligned block of 128 rows (0 to 127, 128 to 255, ...) at most 32 rows name the same one
- route_weight: float32 [2048, 2], P('sp'), may hold values from 0.2 to 1
- w_gate: bfloat16 [16, 2048, 6144], P('sp', None, 'tp'), may hold values from -0.125 to 0.125
- w_up: bfloat16 [16, 2048, 6144], P('sp', None, 'tp'), may hold values from -0.125 to 0.125
- w_down: bfloat16 [16, 6144, 2048], P('sp', 'tp'), may hold values from -0.078125 to 0.078125
- out_proj: bfloat16 [2048, 2048], P('tp'), may hold values from -0.125 to 0.125
- saved_out: bfloat16 [2048, 2048], P('sp', 'tp'), may hold values from -6 to 6
- queries: bfloat16 [2048, 1024], P('sp', 'tp'), may hold values from -6 to 6
- keys: bfloat16 [2048, 1024], P('sp', 'tp'), may hold values from -6 to 6
- values: bfloat16 [2048, 2048], P('sp', 'tp'), may hold values from -6 to 6
- log_decay: float32 [2048, 1024], P('sp', 'tp'), may hold values from -1 to 0
- span_state: float32 [32, 1024, 128], P('sp', 'tp'), may hold values from -6 to 6
Outputs:
- grad_w_gate: bfloat16 [16, 2048, 6144], P('sp', None, 'tp')
- grad_w_up: bfloat16 [16, 2048, 6144], P('sp', None, 'tp')
- grad_w_down: bfloat16 [16, 6144, 2048], P('sp', 'tp')
- grad_proj: float32 [2048, 2048], P('sp', 'tp')
- grad_queries: bfloat16 [2048, 1024], P('sp', 'tp')
- grad_keys: bfloat16 [2048, 1024], P('sp', 'tp')
- grad_values: bfloat16 [2048, 2048], P('sp', 'tp')
- grad_decay: float32 [2048, 1024], P('sp', 'tp')
The draws below stay inside these ranges and needn't reach their ends.
Inputs may be any that keep to these rules, and one draw needn't show every extreme that they name: `route_expert`: each row names two different experts. Within the 128 rows of one index of sp no expert is named by more than 32 rows, a bound that some block reaches.
All inputs are finite; a program needn't handle non-finite values.
Results may differ from the reference program's by a relative error of at most 0.019.
Values may be sent and summed in bfloat16 or wider, within the bound.
A program may use at most 128 MiB of HBM per device.

```python
import math
import jax
import jax.numpy as jnp
import numpy as np
from jax import lax

D = 2048
HEADS = 16
DK = 64
DV = 128
F = 6144
SPAN = 64
TOK_DEV = 128
TOKENS = 2048
EXPERTS = 16
CAP = 32
N_SP = 16


def draw_log_decay(key, part):
    keys_list = jax.random.split(jax.random.fold_in(key, 11), 7)
    channels = HEADS * DK
    fast_variant = jax.random.uniform(keys_list[0], (channels,)) < 0.5
    slow_rate = jnp.log(10.0) / TOKENS * jax.random.uniform(keys_list[1], (channels,), minval=0.1, maxval=0.4)
    quick_rate = 1.0 / jax.random.uniform(keys_list[2], (channels,), minval=30.0, maxval=50.0)
    starting_offset = jnp.where(fast_variant, quick_rate, slow_rate)
    coarse_estimate = jnp.exp(jax.random.uniform(keys_list[3], (TOKENS, channels), minval=-0.7, maxval=0.7))
    levels = jax.random.uniform(keys_list[4], (TOKENS // TOK_DEV, 1, 1), minval=-0.7, maxval=0.7)
    block_multiplier = jnp.exp(jnp.broadcast_to(levels, (TOKENS // TOK_DEV, TOK_DEV, 1)).reshape(TOKENS, 1))
    target_locations = jax.random.randint(keys_list[5], (3,), 0, TOKENS)
    token_locations = jnp.arange(TOKENS, dtype=jnp.int32)
    transfer_group_rows = jnp.any(token_locations[:, None] == target_locations[None, :], axis=1).astype(jnp.float32)
    layer_stack_depth = -jnp.log(jax.random.uniform(keys_list[6], (channels,), minval=0.5, maxval=0.8))
    transfer_group = transfer_group_rows[:, None] * jnp.where(fast_variant, 0.0, layer_stack_depth)[None, :]
    return (-(starting_offset[None, :] * coarse_estimate * block_multiplier) - transfer_group).astype(jnp.float32)


def raised(values, rng, source, target, shards_of, factor):
    owner, partner = [(jnp.arange(values.shape[position]) // (values.shape[position] // shards_of)).reshape([-1 if axis == position else 1 for axis in range(values.ndim)]) for position in (source, target)]
    chosen = jax.random.permutation(rng, shards_of)[partner]
    strong = (owner == chosen) | (owner == (partner + shards_of // 2) % shards_of)
    return jnp.where(strong, factor * values, values)


def shard_levels(stream_key, dims, cuts, low, top_value):
    gain, own = 1.0, jax.random.fold_in(stream_key, 6)
    for position, blocks in cuts:
        heights = jnp.exp(jax.random.uniform(jax.random.fold_in(own, position), (blocks,), jnp.float32, low / len(cuts), top_value / len(cuts)))
        gain = gain * jnp.repeat(heights, dims[position] // blocks).reshape([-1 if axis == position else 1 for axis in range(len(dims))])
    return gain


def routed_block(own_key, own, number, rows, count, top, limit, slope):
    ranking = jax.random.permutation(own_key, count)
    crowded, ordinary = portions_of(count, rows * top, limit, slope, True), portions_of(count, rows * top, limit, slope, False)
    places = jnp.arange(count)

    def named(lengths, offset_by):
        used = int((lengths > 0).sum())
        fixed = max(1, used // 4)
        moved = fixed + (places - fixed + offset_by * (used - fixed)) % max(1, count - fixed)
        return jnp.zeros((count,), jnp.int32).at[ranking[jnp.where(places < fixed, places, moved)]].set(jnp.asarray(lengths, jnp.int32))

    lengths = jnp.where(number % 4 == 0, named(crowded, number // 4), named(ordinary, number - number // 4 - 1))
    mixed = jax.random.permutation(jax.random.fold_in(own, 3), count)
    source_of, taker = mixed[0:count // 2 * 2:2], mixed[1:count // 2 * 2:2]
    room = jnp.minimum(lengths[source_of] - 1, limit - lengths[taker]) // 2
    room = jnp.where((source_of == ranking[0]) | (taker == ranking[0]) | (lengths[taker] == 0), 0, jnp.maximum(room, 0))
    moved = jax.random.randint(jax.random.fold_in(own, 4), (count // 2,), 0, 1 << 20) % (room + 1)
    lengths = lengths.at[source_of].add(-moved).at[taker].add(moved)
    items = jnp.searchsorted(jnp.cumsum(lengths), jnp.arange(rows * top), side="right").astype(jnp.int32)
    table = items.reshape(top, rows).T
    table = table[jax.random.permutation(jax.random.fold_in(own, 1), rows)]
    offset_by = jax.random.randint(jax.random.fold_in(own, 2), (rows, 1), 0, top)
    return jnp.take_along_axis(table, (jnp.arange(top)[None, :] + offset_by) % top, axis=1)


def portions_of(count, total, bound, lean, full):
    loads = [(1 << 20) // math.isqrt(standing ** lean) + 1 for standing in range(1, count + 1)]
    largest = bound if full else min(bound, max(-(-total // count), total * loads[0] // sum(loads)))
    least = 1 if total - largest >= count - 1 else 0
    holding, spare = [largest] + [least] * (count - 1), total - largest - least * (count - 1)
    while spare > 0:
        free = [i for i in range(1, count) if holding[i] < largest] or [i for i in range(1, count) if holding[i] < bound]
        whole, left = sum([loads[i] for i in free]), spare
        for i in free:
            extra = min(bound - holding[i], max(1, left * loads[i] // whole), spare)
            holding[i] = holding[i] + extra
            spare = spare - extra
    return np.array(holding)


def normal_values(rng, extent, spread, most, shards=(), kind=jnp.bfloat16):
    drawn = spread * jax.random.normal(rng, extent, jnp.float32)
    if shards:
        drawn = drawn * shard_levels(rng, extent, shards, -0.22, 0.18)
    return jnp.clip(drawn, -most, most).astype(kind)


def bell_draw_with(own_key, shape, scale, most, cuts, heavy, held_as=jnp.bfloat16):
    values = scale * jax.random.normal(own_key, shape, jnp.float32)
    if cuts:
        values = values * shard_levels(own_key, shape, cuts, -0.22, 0.18)
    return jnp.clip(raised(values, jax.random.fold_in(own_key, 3), *heavy), -most, most).astype(held_as)


def setup_inputs(seed: int = 0) -> dict:
    seeds = jax.random.split(jax.random.key(seed), 15)
    moe_input = normal_values(seeds[0], (TOKENS, D), 1.0, 6.0, ((0, 16),))
    cotangent = bell_draw_with(seeds[1], (TOKENS, D), 1.0, 6.0, ((0, 16),), (0, 1, 16, 2.0))
    route_expert_keys = jax.random.split(jax.random.fold_in(seeds[2], 1), TOKENS // TOK_DEV)
    route_expert_turns = jax.random.permutation(jax.random.fold_in(seeds[2], 3), TOKENS // TOK_DEV)
    route_expert = jax.vmap(lambda own, number: routed_block(jax.random.fold_in(seeds[2], 2), own, number, TOK_DEV, EXPERTS, 2, CAP, 1))(route_expert_keys, route_expert_turns).reshape((TOKENS, 2))
    route_weight = jnp.clip(0.2 + 0.8 * jax.random.uniform(seeds[3], (TOKENS, 2), jnp.float32) ** shard_levels(seeds[3], (TOKENS, 2), ((0, 16),), -0.2, 0.2), 0.2, 1.0)
    w_gate = normal_values(seeds[4], (EXPERTS, D, F), D ** -0.5, 0.125, ((0, 16), (2, 16)))
    w_up = normal_values(seeds[5], (EXPERTS, D, F), D ** -0.5, 0.125, ((0, 16), (2, 16)))
    w_down = normal_values(seeds[6], (EXPERTS, F, D), F ** -0.5, 0.078125, ((0, 16), (1, 16)))
    out_proj = normal_values(seeds[7], (HEADS * DV, D), (HEADS * DV) ** -0.5, 0.125, ((0, 16),))
    saved_out = normal_values(seeds[8], (TOKENS, HEADS * DV), 1.0, 6.0, ((0, 16), (1, 16)))
    queries = normal_values(seeds[9], (TOKENS, HEADS * DK), 1.0, 6.0, ((0, 16), (1, 16)))
    keys = normal_values(seeds[10], (TOKENS, HEADS * DK), 1.0, 6.0, ((0, 16), (1, 16)))
    values = normal_values(seeds[11], (TOKENS, HEADS * DV), 1.0, 6.0, ((0, 16), (1, 16)))
    log_decay = draw_log_decay(jax.random.fold_in(seeds[14], 71), 0)
    span_state = normal_values(seeds[13], (TOKENS // SPAN, HEADS * DK, DV), 1.0, 6.0, ((0, 16), (1, 16)), jnp.float32)
    return {"moe_input": moe_input, "cotangent": cotangent, "route_expert": route_expert, "route_weight": route_weight, "w_gate": w_gate, "w_up": w_up, "w_down": w_down, "out_proj": out_proj, "saved_out": saved_out, "queries": queries, "keys": keys, "values": values, "log_decay": log_decay, "span_state": span_state}


HIGH = lax.Precision.HIGHEST

def slot_places(experts, count):
    routes_flat = experts.reshape(-1)
    one_hot = (routes_flat[:, None] == jnp.arange(count, dtype=jnp.int32)[None, :]).astype(jnp.int32)
    earlier = jnp.cumsum(one_hot, axis=0) - one_hot
    return lax.optimization_barrier(jnp.sum(earlier * one_hot, axis=1)).reshape(experts.shape).astype(jnp.int32)

def expert_grads(inputs, routed, gate_weight, up_weight, down_weight):
    gate = jnp.dot(inputs, gate_weight, preferred_element_type=jnp.float32)
    upper = jnp.dot(inputs, up_weight, preferred_element_type=jnp.float32)
    sigmoid_gate = jax.nn.sigmoid(gate)
    active = gate * sigmoid_gate
    hidden = (active * upper).astype(jnp.bfloat16)
    d_hidden = lax.dot_general(routed, down_weight, (((1,), (1,)), ((), ())), preferred_element_type=jnp.float32)
    d_upper = (d_hidden * active).astype(jnp.bfloat16)
    d_gate = (d_hidden * upper * sigmoid_gate * (1.0 + gate * (1.0 - sigmoid_gate))).astype(jnp.bfloat16)
    grad_down = lax.dot_general(hidden, routed, (((0,), (0,)), ((), ())), preferred_element_type=jnp.float32).astype(jnp.bfloat16)
    grad_gate = lax.dot_general(inputs, d_gate, (((0,), (0,)), ((), ())), preferred_element_type=jnp.float32).astype(jnp.bfloat16)
    grad_up = lax.dot_general(inputs, d_upper, (((0,), (0,)), ((), ())), preferred_element_type=jnp.float32).astype(jnp.bfloat16)
    return (d_gate, d_upper, grad_gate, grad_up, grad_down)

def input_grad(d_gate, d_upper, gate_weight, up_weight):
    first = lax.dot_general(d_gate, gate_weight, (((1,), (1,)), ((), ())), preferred_element_type=jnp.float32)
    second = lax.dot_general(d_upper, up_weight, (((1,), (1,)), ((), ())), preferred_element_type=jnp.float32)
    return first + second

def gated_pieces(queries, keys, values, log_decay, grad_mix, key_dim, span_len):
    value_dim = values.shape[1] * key_dim // queries.shape[1]
    heads = queries.shape[1] // key_dim
    spans = queries.shape[0] // span_len

    def blocks(array, width):
        return array.astype(jnp.float32).reshape(spans, span_len, heads, width)
    query_spans = blocks(queries, key_dim)
    key_spans = blocks(keys, key_dim)
    value_spans = blocks(values, value_dim)
    grad_spans = blocks(grad_mix, value_dim)
    cumulative = jnp.cumsum(blocks(log_decay, key_dim), axis=1)
    last = cumulative[:, -1]
    scale = key_dim ** (-0.5)
    query_decayed = query_spans * jnp.exp(cumulative)
    key_grown = key_spans * jnp.exp(-cumulative)
    key_to_end = key_spans * jnp.exp(last[:, None] - cumulative)
    g_local = scale * jnp.einsum('nthk,nthv->nhkv', query_decayed, grad_spans, precision=HIGH)
    return (query_spans, key_spans, value_spans, grad_spans, cumulative, last, query_decayed, key_grown, key_to_end, g_local)

def backward_step(carry, inputs):
    local, decay = inputs
    return (local + jnp.exp(decay)[..., None] * carry, carry)

def gated_finish(pieces, span_state, g_end, key_dim):
    query_spans, key_spans, value_spans, grad_spans, cumulative, last, query_decayed, key_grown, key_to_end, g_local = pieces
    spans, span_len, heads, value_dim = value_spans.shape
    scale = key_dim ** (-0.5)
    token_locations = jnp.arange(span_len, dtype=jnp.int32)
    causal = (token_locations[:, None] >= token_locations[None, :]).astype(jnp.float32)
    scores = jnp.einsum('nthk,nshk->nhts', query_decayed, key_grown, precision=HIGH) * causal
    grad_dot = jnp.einsum('nthv,nshv->nhts', grad_spans, value_spans, precision=HIGH) * causal
    state = span_state.astype(jnp.float32).reshape(spans, heads, key_dim, value_dim)
    d_query = scale * jnp.exp(cumulative) * (jnp.einsum('nhts,nshk->nthk', grad_dot, key_grown, precision=HIGH) + jnp.einsum('nthv,nhkv->nthk', grad_spans, state, precision=HIGH))
    d_key = scale * jnp.exp(-cumulative) * jnp.einsum('nhts,nthk->nshk', grad_dot, query_decayed, precision=HIGH) + jnp.exp(last[:, None] - cumulative) * jnp.einsum('nshv,nhkv->nshk', value_spans, g_end, precision=HIGH)
    d_value = scale * jnp.einsum('nhts,nthv->nshv', scores, grad_spans, precision=HIGH) + jnp.einsum('nshk,nhkv->nshv', key_to_end, g_end, precision=HIGH)
    state_end = jnp.exp(last)[..., None] * state + jnp.einsum('nshk,nshv->nhkv', key_to_end, value_spans, precision=HIGH)
    tail = lax.optimization_barrier(jnp.sum(state_end * g_end, axis=-1))
    d_cumulative = query_spans * d_query - key_spans * d_key
    d_log = jnp.cumsum(d_cumulative[:, ::-1], axis=1)[:, ::-1] + tail[:, None]
    rows = spans * span_len
    return (d_query.reshape(rows, heads * key_dim).astype(jnp.bfloat16), d_key.reshape(rows, heads * key_dim).astype(jnp.bfloat16), d_value.reshape(rows, heads * value_dim).astype(jnp.bfloat16), d_log.reshape(rows, heads * key_dim))

def place_block(block):
    return slot_places(block, EXPERTS)

def per_expert(items):
    rows_in, rows_cot, gate_weight, up_weight, down_weight = items
    d_gate, d_upper, grad_gate, grad_up, grad_down = expert_grads(rows_in, rows_cot, gate_weight, up_weight, down_weight)
    return (input_grad(d_gate, d_upper, gate_weight, up_weight), grad_gate, grad_up, grad_down)

def reference(moe_input, cotangent, route_expert, route_weight, w_gate, w_up, w_down, out_proj, saved_out, queries, keys, values, log_decay, span_state):
    blocks = route_expert.reshape(N_SP, TOK_DEV, 2)
    target_locations = jax.vmap(place_block)(blocks)
    source = jnp.arange(N_SP, dtype=jnp.int32)[:, None, None]
    slot_index = (blocks * (N_SP * CAP) + source * CAP + target_locations).reshape(-1).astype(jnp.int32)
    owner = jnp.full((EXPERTS * N_SP * CAP,), 2 * TOKENS, jnp.int32).at[slot_index].set(jnp.arange(2 * TOKENS, dtype=jnp.int32))
    weighted = (route_weight[:, :, None] * cotangent[:, None, :].astype(jnp.float32)).astype(jnp.bfloat16)
    weighted = weighted.reshape(2 * TOKENS, D)
    blank = jnp.zeros((1, D), jnp.bfloat16)
    slot_cot = jnp.concatenate([weighted, blank], axis=0)[owner].reshape(EXPERTS, N_SP * CAP, D)
    slot_in = jnp.concatenate([moe_input, blank], axis=0)[owner // 2].reshape(EXPERTS, N_SP * CAP, D)
    slot_grad, grad_w_gate, grad_w_up, grad_w_down = lax.map(per_expert, (slot_in, slot_cot, w_gate, w_up, w_down))
    routed = slot_grad.reshape(-1, D)[slot_index].reshape(TOKENS, 2, D)
    grad_in = (cotangent.astype(jnp.float32) + routed[:, 0] + routed[:, 1]).astype(jnp.bfloat16)
    grad_mix = lax.dot_general(grad_in, out_proj, (((1,), (1,)), ((), ())), preferred_element_type=jnp.float32)
    grad_proj = lax.dot_general(grad_in, saved_out, (((0,), (0,)), ((), ())), preferred_element_type=jnp.float32)
    pieces = gated_pieces(queries, keys, values, log_decay, grad_mix, DK, SPAN)
    g_local = pieces[9]
    last = pieces[5]
    begin = jnp.zeros((HEADS, DK, DV), jnp.float32)
    ignored, g_end = lax.scan(backward_step, begin, (g_local, last), reverse=True)
    grad_queries, grad_keys, grad_values, grad_decay = gated_finish(pieces, span_state, g_end, DK)
    return (grad_w_gate, grad_w_up, grad_w_down, grad_proj, grad_queries, grad_keys, grad_values, grad_decay)
```

```python
import jax
import jax.numpy as jnp
from jax import lax
from jax.sharding import PartitionSpec as P

DK = 64
SPAN = 64


def in_one_piece(arrays, axis, split_dim, concat_dim, along):
    widths = [a.shape[along] for a in arrays]
    both = jnp.concatenate(arrays, axis=along)
    filled = lax.all_to_all(both, axis, split_axis=split_dim, concat_axis=concat_dim, tiled=True)
    return tuple(jnp.split(filled, [sum(widths[:k]) for k in range(1, len(widths))], axis=along))


def over_pieces(shard, axis):
    parts = lax.all_gather(shard, axis).astype(jnp.float32)
    return parts.sum(axis=0)


def in_blocks(shard, dim, length):
    shape = shard.shape
    parts = shard.reshape(*shape[:dim], length, shape[dim] // length, *shape[dim + 1 :])
    return jnp.moveaxis(parts, dim, 0)


def sum_at_owner(shard, axis, dim):
    parts = in_blocks(shard, dim, lax.axis_size(axis))
    arrived = lax.all_to_all(parts, axis, split_axis=0, concat_axis=0, tiled=True)
    return arrived.astype(jnp.float32).sum(axis=0)


def copy_for_each(shard, axis):
    length = lax.axis_size(axis)
    return lax.all_to_all(
        jnp.broadcast_to(shard[None], (length, *shard.shape)), axis, 0, 0, tiled=True
    )


def all_in_one(shard, axis):
    leaves = jax.tree.leaves(shard)
    sequence = sorted(range(len(leaves)), key=lambda k: -leaves[k].size)
    width = (1, *leaves[sequence[0]].shape)[-1]
    lines = [
        jnp.pad(leaves[k].reshape(-1), (0, -leaves[k].size % width)).reshape(-1, width)
        for k in sequence
    ]
    both, at, found = (copy_for_each(jnp.concatenate(lines), axis), 0, {})
    for k, line in zip(sequence, lines):
        slab = both[:, at : at + len(line)].reshape(len(both), -1)
        found[k] = slab[:, : leaves[k].size].reshape(-1, *leaves[k].shape)
        at += len(line)
    numbers = iter(range(len(leaves)))
    return jax.tree.map(lambda _: found[next(numbers)], shard)


def combined_pairwise(pieces, combine):
    while len(jax.tree.leaves(pieces)[0]) > 1:
        pieces = jax.vmap(combine)(
            *(jax.tree.map(lambda part: part[side::2], pieces) for side in (0, 1))
        )
    return jax.tree.map(lambda part: part[0], pieces)


def carried_in(shard, axis, combine, identity):
    length, mine = (lax.axis_size(axis), lax.axis_index(axis))
    passed = jnp.arange(length) > mine

    def kept(part, zero, own):
        part = jnp.where(
            passed.reshape(-1, *(1 for _ in own.shape)), part, jnp.asarray(zero, own.dtype)
        )
        return part[::-1]

    pieces = all_in_one(shard, axis)
    return combined_pairwise(jax.tree.map(kept, pieces, identity, shard), combine)


def slot_places(experts, count):
    routes_flat = experts.reshape(-1)
    one_hot = (routes_flat[:, None] == jnp.arange(count, dtype=jnp.int32)[None, :]).astype(
        jnp.int32
    )
    earlier = jnp.cumsum(one_hot, axis=0) - one_hot
    return jnp.sum(earlier * one_hot, axis=1).reshape(experts.shape)


def expert_grads(inputs, routed, gate_weight, up_weight, down_weight):
    gate = jnp.dot(inputs, gate_weight, preferred_element_type=jnp.float32)
    upper = jnp.dot(inputs, up_weight, preferred_element_type=jnp.float32)
    sigmoid_gate = jax.nn.sigmoid(gate)
    active = gate * sigmoid_gate
    hidden = (active * upper).astype(jnp.bfloat16)
    d_hidden = lax.dot_general(
        routed, down_weight, (((1,), (1,)), ((), ())), preferred_element_type=jnp.float32
    )
    d_upper = (d_hidden * active).astype(jnp.bfloat16)
    d_gate = (d_hidden * upper * sigmoid_gate * (1.0 + gate * (1.0 - sigmoid_gate))).astype(
        jnp.bfloat16
    )
    grad_down = lax.dot_general(
        hidden, routed, (((0,), (0,)), ((), ())), preferred_element_type=jnp.float32
    ).astype(jnp.bfloat16)
    grad_gate = lax.dot_general(
        inputs, d_gate, (((0,), (0,)), ((), ())), preferred_element_type=jnp.float32
    ).astype(jnp.bfloat16)
    grad_up = lax.dot_general(
        inputs, d_upper, (((0,), (0,)), ((), ())), preferred_element_type=jnp.float32
    ).astype(jnp.bfloat16)
    return (d_gate, d_upper, grad_gate, grad_up, grad_down)


def input_grad(d_gate, d_upper, gate_weight, up_weight):
    first = lax.dot_general(
        d_gate, gate_weight, (((1,), (1,)), ((), ())), preferred_element_type=jnp.float32
    )
    second = lax.dot_general(
        d_upper, up_weight, (((1,), (1,)), ((), ())), preferred_element_type=jnp.float32
    )
    return first + second


def gated_pieces(queries, keys, values, log_decay, grad_mix, key_dim, span_len):
    value_dim = values.shape[1] * key_dim // queries.shape[1]
    heads = queries.shape[1] // key_dim
    spans = queries.shape[0] // span_len

    def blocks(array, width):
        return array.astype(jnp.float32).reshape(spans, span_len, heads, width)

    query_spans = blocks(queries, key_dim)
    key_spans = blocks(keys, key_dim)
    value_spans = blocks(values, value_dim)
    grad_spans = blocks(grad_mix, value_dim)
    cumulative = jnp.cumsum(blocks(log_decay, key_dim), axis=1)
    last = cumulative[:, -1]
    scale = key_dim ** (-0.5)
    query_decayed = query_spans * jnp.exp(cumulative)
    key_grown = key_spans * jnp.exp(-cumulative)
    key_to_end = key_spans * jnp.exp(last[:, None] - cumulative)
    g_local = scale * jnp.einsum("nthk,nthv->nhkv", query_decayed, grad_spans)
    return (
        query_spans,
        key_spans,
        value_spans,
        grad_spans,
        cumulative,
        last,
        query_decayed,
        key_grown,
        key_to_end,
        g_local,
    )


def backward_step(carry, inputs):
    local, decay = inputs
    return (local + jnp.exp(decay)[..., None] * carry, carry)


def gated_finish(pieces, span_state, g_end, key_dim):
    (
        query_spans,
        key_spans,
        value_spans,
        grad_spans,
        cumulative,
        last,
        query_decayed,
        key_grown,
        key_to_end,
        g_local,
    ) = pieces
    spans, span_len, heads, value_dim = value_spans.shape
    scale = key_dim ** (-0.5)
    token_locations = jnp.arange(span_len, dtype=jnp.int32)
    causal = (token_locations[:, None] >= token_locations[None, :]).astype(jnp.float32)
    scores = jnp.einsum("nthk,nshk->nhts", query_decayed, key_grown) * causal
    grad_dot = jnp.einsum("nthv,nshv->nhts", grad_spans, value_spans) * causal
    state = span_state.reshape(spans, heads, key_dim, value_dim)
    d_query = (
        scale
        * jnp.exp(cumulative)
        * (
            jnp.einsum("nhts,nshk->nthk", grad_dot, key_grown)
            + jnp.einsum("nthv,nhkv->nthk", grad_spans, state)
        )
    )
    d_key = scale * jnp.exp(-cumulative) * jnp.einsum(
        "nhts,nthk->nshk", grad_dot, query_decayed
    ) + jnp.exp(last[:, None] - cumulative) * jnp.einsum("nshv,nhkv->nshk", value_spans, g_end)
    d_value = scale * jnp.einsum("nhts,nthv->nshv", scores, grad_spans) + jnp.einsum(
        "nshk,nhkv->nshv", key_to_end, g_end
    )
    state_end = jnp.exp(last)[..., None] * state + jnp.einsum(
        "nshk,nshv->nhkv", key_to_end, value_spans
    )
    tail = jnp.sum(state_end * g_end, axis=-1)
    d_cumulative = query_spans * d_query - key_spans * d_key
    d_log = jnp.cumsum(d_cumulative[:, ::-1], axis=1)[:, ::-1] + tail[:, None]
    rows = spans * span_len
    return (
        d_query.reshape(rows, heads * key_dim).astype(jnp.bfloat16),
        d_key.reshape(rows, heads * key_dim).astype(jnp.bfloat16),
        d_value.reshape(rows, heads * value_dim).astype(jnp.bfloat16),
        d_log.reshape(rows, heads * key_dim),
    )


def carry_combine(earlier, later):
    return (later[0] * earlier[0], later[1] + later[0][..., None] * earlier[1])


def on_device(
    moe_input,
    cotangent,
    route_expert,
    route_weight,
    w_gate,
    w_up,
    w_down,
    out_proj,
    saved_out,
    queries,
    keys,
    values,
    log_decay,
    span_state,
):
    tok_rows, width = moe_input.shape
    groups = lax.axis_size("sp")
    lanes = lax.axis_size("tp")
    capacity = 4 * tok_rows // groups
    part = width // lanes
    offset = lax.axis_index("tp") * part
    slots = groups * capacity
    target_locations = slot_places(route_expert, groups)
    slot_index = route_expert * capacity + target_locations
    numbers = jnp.arange(slots, dtype=jnp.int32)
    chosen = [(numbers[:, None] == slot_index[None, :, j]).astype(jnp.bfloat16) for j in (0, 1)]
    my_input = lax.dynamic_slice(moe_input, (0, offset), (tok_rows, part))
    my_cot = lax.dynamic_slice(cotangent, (0, offset), (tok_rows, part))
    weighted = [
        (route_weight[:, j : j + 1] * my_cot.astype(jnp.float32)).astype(jnp.bfloat16)
        for j in (0, 1)
    ]
    send_in = jnp.dot(chosen[0] + chosen[1], my_input, preferred_element_type=jnp.float32)
    send_cot = jnp.dot(
        jnp.concatenate(chosen, axis=1),
        jnp.concatenate(weighted, axis=0),
        preferred_element_type=jnp.float32,
    )
    send = jnp.concatenate([send_in, send_cot], axis=1).astype(jnp.bfloat16)
    got = lax.all_to_all(
        send.reshape(groups, capacity, 2 * part), "sp", split_axis=0, concat_axis=0, tiled=True
    ).reshape(slots, 2 * part)
    rows = lax.all_gather(got, "tp")
    got_in = rows[:, :, :part].transpose(1, 0, 2).reshape(slots, width)
    got_cot = rows[:, :, part:].transpose(1, 0, 2).reshape(slots, width)
    gate_weight = w_gate[0]
    up_weight = w_up[0]
    down_weight = w_down[0]
    d_gate, d_upper, grad_gate, grad_up, grad_down = expert_grads(
        got_in, got_cot, gate_weight, up_weight, down_weight
    )
    partial_value = input_grad(d_gate, d_upper, gate_weight, up_weight).astype(jnp.bfloat16)
    mine = lax.psum_scatter(partial_value, "tp", scatter_dimension=1, tiled=True)
    returned = lax.all_to_all(
        mine.reshape(groups, capacity, part), "sp", split_axis=0, concat_axis=0, tiled=True
    ).reshape(slots, part)
    routed = lax.dot_general(
        chosen[0] + chosen[1],
        returned,
        (((0,), (0,)), ((), ())),
        preferred_element_type=jnp.float32,
    )
    grad_in = (my_cot.astype(jnp.float32) + routed).astype(jnp.bfloat16)
    grad_in = lax.all_gather(grad_in, "tp", axis=1, tiled=True)
    grad_mix = lax.dot_general(
        grad_in, out_proj, (((1,), (1,)), ((), ())), preferred_element_type=jnp.float32
    )
    grad_proj = sum_at_owner(
        lax.dot_general(
            grad_in, saved_out, (((0,), (0,)), ((), ())), preferred_element_type=jnp.float32
        ).astype(jnp.bfloat16),
        "sp",
        0,
    )
    pieces = gated_pieces(queries, keys, values, log_decay, grad_mix, DK, SPAN)
    g_local = pieces[9]
    last = pieces[5]
    begin = jnp.zeros(g_local.shape[1:], jnp.float32)
    device_start, local_end = lax.scan(backward_step, begin, (g_local, last), reverse=True)
    device_decay = jnp.exp(jnp.sum(last, axis=0))
    identity = (jnp.ones_like(device_decay), jnp.zeros_like(device_start))
    decay_after, state_after = carried_in(
        (device_decay, device_start), "sp", carry_combine, identity
    )
    running = jnp.cumsum(last, axis=0)
    beyond = running[-1][None] - running
    g_end = local_end + jnp.exp(beyond)[..., None] * state_after[None]
    grad_queries, grad_keys, grad_values, grad_decay = gated_finish(pieces, span_state, g_end, DK)
    return (
        grad_gate[None],
        grad_up[None],
        grad_down[None],
        grad_proj,
        grad_queries,
        grad_keys,
        grad_values,
        grad_decay,
    )


def solution(mesh):
    placed = (
        P("sp", None),
        P("sp", None),
        P("sp", None),
        P("sp", None),
        P("sp", None, "tp"),
        P("sp", None, "tp"),
        P("sp", "tp", None),
        P("tp", None),
        P("sp", "tp"),
        P("sp", "tp"),
        P("sp", "tp"),
        P("sp", "tp"),
        P("sp", "tp"),
        P("sp", "tp", None),
    )
    return jax.shard_map(
        on_device,
        mesh=mesh,
        in_specs=placed,
        out_specs=(
            P("sp", None, "tp"),
            P("sp", None, "tp"),
            P("sp", "tp", None),
            P("sp", "tp"),
            P("sp", "tp"),
            P("sp", "tp"),
            P("sp", "tp"),
            P("sp", "tp"),
        ),
        check_vma=False,
    )
```

```python
import functools

import jax
import jax.numpy as jnp
from jax import lax
from jax.experimental import pallas as pl
from jax.experimental.pallas import tpu as pltpu
from jax.sharding import PartitionSpec as P

BF = jnp.bfloat16
F32 = jnp.float32
HIGH = lax.Precision.HIGHEST
LANE = 128
DK = 64
SPAN = 64
NN = (((1,), (0,)), ((), ()))
NT = (((1,), (1,)), ((), ()))
TN = (((0,), (0,)), ((), ()))


def mm(a, b, dims=NN, precision=None):
    return lax.dot_general(a, b, dims, precision=precision, preferred_element_type=F32)


def half_dot(a, b, dims=NN):
    return mm(a.astype(BF), b.astype(BF), dims)


def waited(ref, sem):
    pltpu.make_async_copy(ref, ref, sem).wait()


def main_kernel(
    route_ref, weight_ref, input_ref, cot_ref, proj_ref, saved_ref, q_ref, k_ref, v_ref, log_ref,
    state_ref, wg_hbm, wu_hbm, wd_hbm,
    rows_hbm, hid_hbm, dg_hbm, du_hbm, gproj_ref, gq_ref, gk_ref, gv_ref, gd_ref,
    wg, wu, wd, table, send, rows, gate_acc, up_acc, hid_acc, hid, dgu, tmp, mine, pair_out,
    pair_in, back_out, back_in, far_out, far_in, grad_in, pj_out, pj_in, pj_own, tot_out, tot_in,
    carry_out, carry_in, after,
    w_sem, out_sem, disp_s, disp_r, ring_s, ring_r, core_s, core_r, pair_s, pair_r, back_s, back_r,
    far_s, far_r, all_s, all_r, fwd_s, fwd_r, pj_s, pj_r, tot_s, tot_r, carry_s, carry_r,
    *, groups, lanes, capacity,
):
    chips = lanes // 2
    sp, tp = lax.axis_index("sp"), lax.axis_index("tp")
    z, core = lax.div(tp, 2), lax.rem(tp, 2)
    other = 1 - core
    tokens = input_ref.shape[0]
    slots = groups * capacity
    hidden = wg.shape[1]
    half = groups // 2

    def wrapped(rel):
        return lax.rem(z + rel, chips)

    def to(src, dst, send_sem, recv_sem, **where):
        pltpu.make_async_remote_copy(
            src_ref=src, dst_ref=dst, send_sem=send_sem, recv_sem=recv_sem,
            device_id=where, device_id_type=pl.DeviceIdType.MESH,
        ).start()

    def to_tp(src, dst, send_sem, recv_sem, chip, at_core):
        to(src, dst, send_sem, recv_sem, tp=chip * 2 + at_core)

    barrier = pltpu.get_barrier_semaphore()

    @pl.loop(1, groups)
    def _(o):
        pl.semaphore_signal(
            barrier, inc=1, device_id={"sp": lax.rem(sp + o, groups)},
            device_id_type=pl.DeviceIdType.MESH,
        )

    @pl.loop(1, chips)
    def _(o):
        pl.semaphore_signal(
            barrier, inc=1, device_id={"tp": wrapped(o) * 2 + core},
            device_id_type=pl.DeviceIdType.MESH,
        )

    pl.semaphore_signal(
        barrier, inc=1, device_id={"tp": z * 2 + other}, device_id_type=pl.DeviceIdType.MESH
    )

    copies = [
        pltpu.make_async_copy(wg_hbm.at[0], wg, w_sem.at[0]),
        pltpu.make_async_copy(wu_hbm.at[0], wu, w_sem.at[1]),
        pltpu.make_async_copy(wd_hbm.at[0], wd, w_sem.at[2]),
    ]
    for copy in copies:
        copy.start()

    experts = lax.broadcasted_iota(jnp.int32, (tokens, groups), 1)
    named = [(route_ref[:, j : j + 1] == experts).astype(F32) for j in (0, 1)]
    row = lax.broadcasted_iota(jnp.int32, (tokens, tokens), 0)
    col = lax.broadcasted_iota(jnp.int32, (tokens, tokens), 1)
    earlier = half_dot((row > col).astype(F32), named[0] + named[1])
    place_in = lax.broadcasted_iota(jnp.int32, (tokens, slots), 1)
    for j in (0, 1):
        place = jnp.sum(earlier * named[j], axis=1, keepdims=True).astype(jnp.int32)
        slot = route_ref[:, j : j + 1] * capacity + place
        table[j] = (slot == place_in).astype(F32).astype(BF)
    far_blocks = list(range(3, chips - 2)) if chips > 4 else [2]
    near = 2 if chips > 4 else 1
    firsts = [0] + far_blocks

    def fill(b, rel):
        t = wrapped(rel) * 2 + core
        columns = pl.ds(pl.multiple_of(t * LANE, LANE), LANE)
        cot = cot_ref[:, columns].astype(F32)
        first = table[0]
        second = table[1]
        ins = mm(first + second, input_ref[:, columns], TN)
        cots = mm(first, (weight_ref[:, 0:1] * cot).astype(BF), TN)
        cots += mm(second, (weight_ref[:, 1:2] * cot).astype(BF), TN)
        send[b, :, :capacity] = ins.astype(BF).reshape(groups, capacity, LANE)
        send[b, :, capacity:] = cots.astype(BF).reshape(groups, capacity, LANE)
        rows[t, sp] = send[b, sp]

    def dispatch(b, rel):
        t = wrapped(rel) * 2 + core

        @pl.loop(1, groups)
        def _(o):
            peer = lax.rem(sp + o, groups)
            to(send.at[b, peer], rows.at[t, sp], disp_s.at[b], disp_r.at[b], sp=peer)

    fill(0, 0)
    totals = jnp.sum(log_ref[...], axis=0, keepdims=True)
    tot_out[...] = jnp.concatenate(
        [jnp.broadcast_to(totals, (8, DK)), jnp.zeros((8, LANE - DK), F32)], axis=1
    )
    tot_in[sp] = tot_out[...]
    pl.semaphore_wait(barrier, groups - 1 + chips)

    dispatch(0, 0)
    for b, rel in enumerate(firsts):
        if b:
            fill(b, rel)
            dispatch(b, rel)

    @pl.loop(1, groups)
    def _(o):
        peer = lax.rem(sp + o, groups)
        to(tot_out, tot_in.at[sp], tot_s, tot_r, sp=peer)

    gate_acc[...] = jnp.zeros_like(gate_acc)
    up_acc[...] = jnp.zeros_like(up_acc)
    hid_acc[...] = jnp.zeros_like(hid_acc)

    def halves(t, h):
        return rows.at[t, pl.ds(h * half, half)]

    def block(rel):
        return wrapped(rel) * 2 + core

    def pass_ring(rel, step, h, side):
        chip = wrapped(1 if side == 0 else chips - 1)
        part = halves(block(rel), h)
        to_tp(part, part, ring_s.at[step, side, h], ring_r.at[step, side, h], chip, core)

    def await_ring(rel, step, h, side):
        waited(halves(block(rel), h), ring_r.at[step, side, h])

    def to_other(rel):
        t = block(rel)
        to_tp(rows.at[t], rows.at[t], core_s.at[rel], core_r.at[rel], z, other)

    def from_other(rel):
        waited(rows.at[wrapped(rel) * 2 + other], core_r.at[rel])

    def both(zz, start):
        pieces = [
            rows[zz * 2 + k, :, start : start + capacity].reshape(slots, LANE) for k in (0, 1)
        ]
        return jnp.concatenate(pieces, axis=1)

    def gather_product(rel):
        zz = wrapped(rel)
        depth = pl.ds(pl.multiple_of(zz * 2 * LANE, 2 * LANE), 2 * LANE)
        ins = both(zz, 0)
        gate_acc[...] += mm(ins, wg[depth, :])
        up_acc[...] += mm(ins, wu[depth, :])
        hid_acc[...] += mm(both(zz, capacity), wd[:, depth], NT)

    def await_dispatch(b):
        waited(send.at[b, pl.ds(0, groups - 1)], disp_r.at[b])

    await_dispatch(0)
    for h in (0, 1):
        for side in (0, 1):
            pass_ring(0, 0, h, side)
    to_other(0)
    for copy in copies:
        copy.wait()
    from_other(0)
    gather_product(0)
    for h in (0, 1):
        for side in (0, 1):
            rel = chips - 1 if side == 0 else 1
            await_ring(rel, 0, h, side)
            if near > 1:
                pass_ring(rel, 1, h, side)
        if h == 0 and len(firsts) > 1:
            await_dispatch(1)
            to_other(firsts[1])
    to_other(1)
    to_other(chips - 1)
    for b, rel in enumerate(firsts):
        if b > 1:
            await_dispatch(b)
            to_other(rel)

    @pl.loop(0, len(far_blocks))
    def _(i):
        rel = far_blocks[0] + i
        from_other(rel)
        gather_product(rel)

    @pl.loop(0, 2)
    def _(i):
        rel = 1 + i * (chips - 2)
        from_other(rel)
        gather_product(rel)

    if near > 1:
        for side in (0, 1):
            rel = chips - 2 if side == 0 else 2
            for h in (0, 1):
                await_ring(rel, 1, h, side)
            to_other(rel)

        @pl.loop(0, 2)
        def _(i):
            rel = chips - 2 - i * (chips - 4)
            from_other(rel)
            gather_product(rel)

    rows_copy = pltpu.make_async_copy(rows, rows_hbm, out_sem.at[0])
    rows_copy.start()
    tile = 64

    @pl.loop(0, slots // tile)
    def _(i):
        at = pl.ds(pl.multiple_of(i * tile, tile), tile)
        gate = gate_acc[at, :]
        upper = up_acc[at, :]
        d_hidden = hid_acc[at, :]
        sigmoid = jax.nn.sigmoid(gate)
        active = gate * sigmoid
        hid[at, :] = (active * upper).astype(BF)
        dgu[at, hidden:] = (d_hidden * active).astype(BF)
        dgu[at, :hidden] = (
            d_hidden * upper * sigmoid * (1.0 + gate * (1.0 - sigmoid))
        ).astype(BF)

    out_copies = [
        pltpu.make_async_copy(hid, hid_hbm, out_sem.at[1]),
        pltpu.make_async_copy(dgu.at[:, pl.ds(0, hidden)], dg_hbm, out_sem.at[2]),
        pltpu.make_async_copy(dgu.at[:, pl.ds(hidden, hidden)], du_hbm, out_sem.at[3]),
    ]
    for copy in out_copies:
        copy.start()

    def far_first(j):
        return lax.rem(chips // 2 + lax.div(j + 1, 2) * (2 * lax.rem(j, 2) - 1), chips)

    def slot_block(j):
        zz = wrapped(far_first(j))
        depth = pl.ds(pl.multiple_of(zz * 2 * LANE, 2 * LANE), 2 * LANE)
        tmp[...] = mm(dgu[:, :hidden], wg[depth, :], NT) + mm(dgu[:, hidden:], wu[depth, :], NT)
        pair_out[j] = tmp[:, pl.ds(pl.multiple_of(other * LANE, LANE), LANE)].astype(BF)
        mine[j] = tmp[:, pl.ds(pl.multiple_of(core * LANE, LANE), LANE)]
        to_tp(pair_out.at[j], pair_in.at[j], pair_s.at[j], pair_r.at[j], z, other)

    def slot_return(j):
        waited(pair_in.at[j], pair_r.at[j])
        whole = (mine[j] + pair_in[j].astype(F32)).astype(BF)
        back_out[j] = whole.reshape(groups, capacity, LANE)
        back_in[j, sp] = back_out[j, sp]

        @pl.loop(1, groups)
        def _(o):
            peer = lax.rem(sp + o, groups)
            to(back_out.at[j, peer], back_in.at[j, sp], back_s.at[j], back_r.at[j], sp=peer)

    lag = 2

    @pl.loop(0, chips + lag)
    def _(j):
        @pl.when(j < chips)
        def _():
            slot_block(j)

        @pl.when(j >= lag)
        def _():
            slot_return(j - lag)

    def routed(j):
        waited(back_out.at[j, pl.ds(0, groups - 1)], back_r.at[j])
        return mm(table[0] + table[1], back_in[j].reshape(slots, LANE))

    @pl.loop(0, chips - 1)
    def _(j):
        rel = far_first(j)
        far_out[j] = routed(j).astype(BF)
        to_tp(far_out.at[j], far_in.at[rel], far_s.at[j], far_r.at[rel], wrapped(rel), core)

    total = routed(chips - 1)
    causal = ((row >= col) & (lax.div(row, SPAN) == lax.div(col, SPAN))).astype(F32)
    cum = mm(causal, log_ref[...], NN, HIGH)
    cum_t = mm(log_ref[...], causal, (((0,), (1,)), ((), ())), HIGH)
    waited(tot_in.at[pl.ds(0, groups - 1)], tot_r)
    after_row = lax.broadcasted_iota(jnp.int32, (groups, LANE), 0)
    after_col = lax.broadcasted_iota(jnp.int32, (groups, LANE), 1)
    between = ((after_row > after_col) & (after_row < sp)).astype(F32)
    factors = jnp.exp(mm(tot_in[:, 0, :DK], between, TN, HIGH))

    for rel in range(1, chips):
        waited(far_in.at[rel], far_r.at[rel])
        total += far_in[rel].astype(F32)
    columns = pl.ds(pl.multiple_of(tp * LANE, LANE), LANE)
    grad_in[tp] = (cot_ref[:, columns].astype(F32) + total).astype(BF)
    order = sorted(range(1, chips), key=lambda r: -min(r, chips - r))
    for rel in order:
        to_tp(grad_in.at[tp], grad_in.at[tp], all_s.at[rel], all_r.at[rel], wrapped(rel), core)
    to_tp(grad_in.at[tp], grad_in.at[tp], fwd_s.at[0], fwd_r.at[0], z, other)
    for rel in order[::-1]:
        t = wrapped(chips - rel) * 2 + core
        waited(grad_in.at[t], all_r.at[rel])
        to_tp(grad_in.at[t], grad_in.at[t], fwd_s.at[rel], fwd_r.at[rel], z, other)
    for rel in range(chips):
        waited(grad_in.at[wrapped(chips - rel if rel else 0) * 2 + other], fwd_r.at[rel])

    mix = jnp.zeros((tokens, LANE), F32)
    for zz in range(chips):
        pair = jnp.concatenate([grad_in[2 * zz], grad_in[2 * zz + 1]], axis=1)
        mix += mm(pair, proj_ref[:, 2 * zz * LANE : 2 * (zz + 1) * LANE], NT)

    scale = DK ** (-0.5)
    grown = jnp.exp(cum)
    shrunk = jnp.exp(-cum)
    queries = q_ref[...].astype(F32)
    keys = k_ref[...].astype(F32)
    qd = (queries * grown).astype(BF)
    kd = (keys * shrunk).astype(BF)
    mix_half = mix.astype(BF)
    spans = [slice(n * SPAN, (n + 1) * SPAN) for n in (0, 1)]
    local = [scale * mm(qd[s], mix_half[s], TN) for s in spans]
    last_t = [jnp.exp(cum_t[:, n * SPAN + SPAN - 1 : (n + 1) * SPAN]) for n in (0, 1)]
    begin = local[0] + last_t[0] * local[1]
    for r in range(groups - 1):
        @pl.when(sp > r)
        def _():
            carry_out[r] = (begin * factors[:, r : r + 1]).astype(BF)
            to(carry_out.at[r], carry_in.at[sp], carry_s.at[r], carry_r.at[sp], sp=r)

    @pl.loop(1, groups)
    def _(o):
        peer = lax.rem(sp + o, groups)
        pj_out[peer] = mm(grad_in[peer], saved_ref[...], TN).astype(BF)
        to(pj_out.at[peer], pj_in.at[sp], pj_s, pj_r, sp=peer)

    pj_own[...] = mm(grad_in[sp], saved_ref[...], TN)

    values = v_ref[...]
    ends = [cum[n * SPAN + SPAN - 1 : (n + 1) * SPAN] for n in (0, 1)]
    to_end = [jnp.exp(ends[n] - cum[spans[n]]) for n in (0, 1)]
    ke = [(keys[spans[n]] * to_end[n]).astype(BF) for n in (0, 1)]
    lower = causal[:SPAN, :SPAN]
    parts = []
    for n in (0, 1):
        s = spans[n]
        state = state_ref[n]
        scores = mm(qd[s], kd[s], NT) * lower
        dots = (mm(mix_half[s], values[s], NT) * lower).astype(BF)
        dq = scale * grown[s] * (mm(dots, kd[s]) + mm(mix_half[s], state.astype(BF), NT))
        dk = scale * shrunk[s] * mm(dots, qd[s], TN)
        dv = scale * mm(scores.astype(BF), mix_half[s], TN)
        state_end = last_t[n] * state + mm(ke[n], values[s], TN)
        parts.append((dq, dk, dv, state_end))

    after[...] = jnp.zeros_like(after)
    for s in range(1, groups):
        @pl.when(s > sp)
        def _():
            waited(carry_in.at[s], carry_r.at[s])
            after[...] += carry_in[s].astype(F32)

    end_1 = after[...]
    g_end = [local[1] + last_t[1] * end_1, end_1]
    upper_ones = (col[:SPAN, :SPAN] >= row[:SPAN, :SPAN]).astype(F32)
    for n in (0, 1):
        s = spans[n]
        dq, dk, dv, state_end = parts[n]
        end = g_end[n].astype(BF)
        dk = dk + to_end[n] * mm(values[s], end, NT)
        dv = dv + mm(ke[n], end)
        tail = mm(jnp.ones((8, LANE), F32), state_end * g_end[n], NT, HIGH)[:1]
        d_cum = queries[s] * dq - keys[s] * dk
        gd_ref[s, :] = mm(upper_ones, d_cum, NN, HIGH) + tail
        gq_ref[s, :] = dq.astype(BF)
        gk_ref[s, :] = dk.astype(BF)
        gv_ref[s, :] = dv.astype(BF)

    waited(pj_in.at[pl.ds(0, groups - 1)], pj_r)
    gproj_ref[...] = pj_own[...]

    @pl.loop(1, groups)
    def _(o):
        peer = lax.rem(sp + o, groups)
        gproj_ref[...] += pj_in[peer].astype(F32)

    for b in range(len(firsts)):
        waited(send.at[b, pl.ds(0, groups - 1)], disp_s.at[b])
    waited(tot_in.at[pl.ds(0, groups - 1)], tot_s)
    for step in range(near):
        for side in (0, 1):
            for h in (0, 1):
                waited(halves(0, h), ring_s.at[step, side, h])
    for rel in range(chips):
        waited(rows.at[0], core_s.at[rel])
        waited(pair_out.at[rel], pair_s.at[rel])
        waited(back_out.at[rel, pl.ds(0, groups - 1)], back_s.at[rel])
        waited(grad_in.at[0], fwd_s.at[rel])
        if rel:
            waited(far_out.at[0], far_s.at[rel - 1])
            waited(grad_in.at[0], all_s.at[rel])
    waited(pj_out.at[pl.ds(0, groups - 1)], pj_s)
    for r in range(groups - 1):
        @pl.when(sp > r)
        def _():
            waited(carry_out.at[r], carry_s.at[r])
    rows_copy.wait()
    for copy in out_copies:
        copy.wait()


def weight_kernel(rows, hid, dg, du, gp, gq, gk, gv, gd, gg, gu, gw, op, oq, ok, ov, od):
    slots = hid.shape[0]
    capacity = rows.shape[2] // 2

    def both(start):
        pieces = [rows[k, :, start : start + capacity].reshape(slots, LANE) for k in (0, 1)]
        return jnp.concatenate(pieces, axis=1)

    ins = both(0)
    gg[0] = mm(ins, dg[...], TN).astype(BF)
    gu[0] = mm(ins, du[...], TN).astype(BF)
    gw[0] = mm(hid[...], both(capacity), TN).astype(BF)

    @pl.when(pl.program_id(0) == 0)
    def _():
        for out, given in ((op, gp), (oq, gq), (ok, gk), (ov, gv), (od, gd)):
            out[...] = given[...]


def on_device(
    moe_input, cotangent, route_expert, route_weight, w_gate, w_up, w_down, out_proj, saved_out,
    queries, keys, values, log_decay, span_state,
):
    groups, lanes = lax.axis_size("sp"), lax.axis_size("tp")
    tokens, width = moe_input.shape
    capacity = 4 * tokens // groups
    slots = groups * capacity
    hidden = w_gate.shape[2]
    chips = lanes // 2
    firsts = 4 if chips > 4 else 2
    vmem = pl.BlockSpec(memory_space=pltpu.VMEM)
    hbm = pl.BlockSpec(memory_space=pl.ANY)
    dma = pltpu.SemaphoreType.DMA
    shape = jax.ShapeDtypeStruct
    slab = (groups, 2 * capacity, LANE)
    scratch = [
        pltpu.VMEM((width, hidden), BF),
        pltpu.VMEM((width, hidden), BF),
        pltpu.VMEM((hidden, width), BF),
        pltpu.VMEM((2, tokens, slots), BF),
        pltpu.VMEM((firsts, *slab), BF),
        pltpu.VMEM((lanes, *slab), BF),
        pltpu.VMEM((slots, hidden), F32),
        pltpu.VMEM((slots, hidden), F32),
        pltpu.VMEM((slots, hidden), F32),
        pltpu.VMEM((slots, hidden), BF),
        pltpu.VMEM((slots, 2 * hidden), BF),
        pltpu.VMEM((slots, 2 * LANE), F32),
        pltpu.VMEM((chips, slots, LANE), F32),
        pltpu.VMEM((chips, slots, LANE), BF),
        pltpu.VMEM((chips, slots, LANE), BF),
        pltpu.VMEM((chips, groups, capacity, LANE), BF),
        pltpu.VMEM((chips, groups, capacity, LANE), BF),
        pltpu.VMEM((chips, tokens, LANE), BF),
        pltpu.VMEM((chips, tokens, LANE), BF),
        pltpu.VMEM((lanes, tokens, LANE), BF),
        pltpu.VMEM((groups, LANE, LANE), BF),
        pltpu.VMEM((groups, LANE, LANE), BF),
        pltpu.VMEM((LANE, LANE), F32),
        pltpu.VMEM((8, LANE), F32),
        pltpu.VMEM((groups, 8, LANE), F32),
        pltpu.VMEM((groups, DK, LANE), BF),
        pltpu.VMEM((groups, DK, LANE), BF),
        pltpu.VMEM((DK, LANE), F32),
        dma((3,)), dma((4,)),
        dma((firsts,)), dma((firsts,)),
        dma((2, 2, 2)), dma((2, 2, 2)),
        dma((chips,)), dma((chips,)),
        dma((chips,)), dma((chips,)),
        dma((chips,)), dma((chips,)),
        dma((chips,)), dma((chips,)),
        dma((chips,)), dma((chips,)),
        dma((chips,)), dma((chips,)),
        dma, dma, dma, dma,
        dma((groups,)), dma((groups,)),
    ]
    rows, hid, dg, du, gp, gq, gk, gv, gd = pl.pallas_call(
        functools.partial(main_kernel, groups=groups, lanes=lanes, capacity=capacity),
        name="experts_and_attention",
        out_shape=(
            shape((lanes, *slab), BF),
            shape((slots, hidden), BF),
            shape((slots, hidden), BF),
            shape((slots, hidden), BF),
            shape((LANE, LANE), F32),
            shape((tokens, DK), BF),
            shape((tokens, DK), BF),
            shape((tokens, LANE), BF),
            shape((tokens, DK), F32),
        ),
        in_specs=[vmem] * 11 + [hbm] * 3,
        out_specs=(hbm,) * 4 + (vmem,) * 5,
        scratch_shapes=scratch,
        compiler_params=pltpu.CompilerParams(
            collective_id=0, has_side_effects=True, vmem_limit_bytes=56 * 1024 * 1024
        ),
    )(
        route_expert, route_weight, moe_input, cotangent, out_proj, saved_out, queries, keys,
        values, log_decay, span_state, w_gate, w_up, w_down,
    )
    small = (gp, gq, gk, gv, gd)

    def same(array):
        return pl.BlockSpec(array.shape, lambda i: (0,) * array.ndim)

    results = pl.pallas_call(
        weight_kernel,
        name="weight_grads",
        grid=(chips,),
        out_shape=(
            shape((1, width, hidden), BF),
            shape((1, width, hidden), BF),
            shape((1, hidden, width), BF),
            *(shape(a.shape, a.dtype) for a in small),
        ),
        in_specs=[
            pl.BlockSpec((2, *slab), lambda i: (i, 0, 0, 0)),
            *(same(a) for a in (hid, dg, du, *small)),
        ],
        out_specs=(
            pl.BlockSpec((1, 2 * LANE, hidden), lambda i: (0, i, 0)),
            pl.BlockSpec((1, 2 * LANE, hidden), lambda i: (0, i, 0)),
            pl.BlockSpec((1, hidden, 2 * LANE), lambda i: (0, 0, i)),
            *(same(a) for a in small),
        ),
        compiler_params=pltpu.CompilerParams(vmem_limit_bytes=32 * 1024 * 1024),
    )(rows, hid, dg, du, *small)
    return results


def solution(mesh):
    placed = (
        P("sp", None),
        P("sp", None),
        P("sp", None),
        P("sp", None),
        P("sp", None, "tp"),
        P("sp", None, "tp"),
        P("sp", "tp", None),
        P("tp", None),
        P("sp", "tp"),
        P("sp", "tp"),
        P("sp", "tp"),
        P("sp", "tp"),
        P("sp", "tp"),
        P("sp", "tp", None),
    )
    return jax.shard_map(
        on_device,
        mesh=mesh,
        in_specs=placed,
        out_specs=(
            P("sp", None, "tp"),
            P("sp", None, "tp"),
            P("sp", "tp", None),
            P("sp", "tp"),
            P("sp", "tp"),
            P("sp", "tp"),
            P("sp", "tp"),
            P("sp", "tp"),
        ),
        check_vma=False,
    )
```

```python
import functools

import jax
import jax.numpy as jnp
from jax import lax
from jax.experimental import pallas as pl
from jax.experimental.pallas import tpu as pltpu
from jax.sharding import PartitionSpec as P

BF = jnp.bfloat16
F32 = jnp.float32
HIGH = lax.Precision.HIGHEST
LANE = 128
DK = 64
SPAN = 64
NN = (((1,), (0,)), ((), ()))
NT = (((1,), (1,)), ((), ()))
TN = (((0,), (0,)), ((), ()))


def mm(a, b, dims=NN, precision=None):
    return lax.dot_general(a, b, dims, precision=precision, preferred_element_type=F32)


def half_dot(a, b, dims=NN):
    return mm(a.astype(BF), b.astype(BF), dims)


def waited(ref, sem):
    pltpu.make_async_copy(ref, ref, sem).wait()


def main_kernel(
    route_hbm, weight_hbm, input_hbm, cot_hbm, proj_hbm, saved_hbm, q_hbm, k_hbm, v_hbm, log_hbm,
    state_hbm, wg_hbm, wu_hbm, wd_hbm,
    gg_ref, gu_ref, gw_ref, gproj_ref, gq_ref, gk_ref, gv_ref, gd_ref,
    route_ref, weight_ref, input_ref, cot_ref, proj_ref, saved_ref, q_ref, k_ref, v_ref, log_ref,
    state_ref, wgu, wd, rows, hid_t, dgu, table, picks, send, gu_acc, hid_acc, tmp, mine, pair_out,
    pair_in, near_out, near_in, back_out, back_in, far_out, far_in, grad_in, all_in, all_saved,
    tot_out, tot_in,
    carry_out, carry_in, after,
    w_sem, load_sem, disp_s, disp_r, ring_s, ring_r, core_s, core_r, pair_s, pair_r, near_s, near_r, back_s, back_r,
    far_s, far_r, all_s, all_r, fwd_s, fwd_r, save_s, save_r, opp_s, opp_r, mate_s, mate_r, pj_s, pj_r, tot_s, tot_r, carry_s, carry_r,
    *, groups, lanes, capacity,
):
    chips = lanes // 2
    sp, tp = lax.axis_index("sp"), lax.axis_index("tp")
    z, core = lax.div(tp, 2), lax.rem(tp, 2)
    other = 1 - core
    tokens = input_ref.shape[0]
    slots = groups * capacity
    hidden = wd.shape[0]
    half = groups // 2

    def wrapped(rel):
        return lax.rem(z + rel, chips)

    def to(src, dst, send_sem, recv_sem, **where):
        pltpu.make_async_remote_copy(
            src_ref=src, dst_ref=dst, send_sem=send_sem, recv_sem=recv_sem,
            device_id=where, device_id_type=pl.DeviceIdType.MESH,
        ).start()

    def to_tp(src, dst, send_sem, recv_sem, chip, at_core):
        to(src, dst, send_sem, recv_sem, tp=chip * 2 + at_core)

    barrier = pltpu.get_barrier_semaphore()

    @pl.loop(1, groups)
    def _(o):
        pl.semaphore_signal(
            barrier, inc=1, device_id={"sp": lax.rem(sp + o, groups)},
            device_id_type=pl.DeviceIdType.MESH,
        )

    @pl.loop(1, chips)
    def _(o):
        pl.semaphore_signal(
            barrier, inc=1, device_id={"tp": wrapped(o) * 2 + core},
            device_id_type=pl.DeviceIdType.MESH,
        )

    pl.semaphore_signal(
        barrier, inc=1, device_id={"tp": z * 2 + other}, device_id_type=pl.DeviceIdType.MESH
    )

    given = [
        route_hbm, weight_hbm, input_hbm, cot_hbm, log_hbm, proj_hbm, saved_hbm, q_hbm, k_hbm,
        v_hbm, state_hbm,
    ]
    held = [
        route_ref, weight_ref, input_ref, cot_ref, log_ref, proj_ref, saved_ref, q_ref, k_ref,
        v_ref, state_ref,
    ]
    loads = [
        pltpu.make_async_copy(src, dst, load_sem.at[n])
        for n, (src, dst) in enumerate(zip(given, held))
    ]
    for copy in loads[:5]:
        copy.start()
    copies = [
        pltpu.make_async_copy(wg_hbm.at[0], wgu.at[:, pl.ds(0, hidden)], w_sem.at[0]),
        pltpu.make_async_copy(wu_hbm.at[0], wgu.at[:, pl.ds(hidden, hidden)], w_sem.at[1]),
        pltpu.make_async_copy(wd_hbm.at[0], wd, w_sem.at[2]),
    ]
    for copy in loads[:2]:
        copy.wait()
    experts = lax.broadcasted_iota(jnp.int32, (groups, tokens), 0)
    named = [(route_ref[j : j + 1, :] == experts).astype(F32) for j in (0, 1)]
    row = lax.broadcasted_iota(jnp.int32, (tokens, tokens), 0)
    col = lax.broadcasted_iota(jnp.int32, (tokens, tokens), 1)
    earlier = half_dot(named[0] + named[1], (row < col).astype(F32))
    place_in = lax.broadcasted_iota(jnp.int32, (slots, tokens), 0)
    found = []
    for j in (0, 1):
        place = jnp.sum(earlier * named[j], axis=0, keepdims=True).astype(jnp.int32)
        slot = route_ref[j : j + 1, :] * capacity + place
        found.append((slot == place_in).astype(F32))
        table[:, j * tokens : (j + 1) * tokens] = found[j].astype(BF)
    picks[...] = jnp.transpose(found[0] + found[1]).astype(BF)
    weights = jnp.transpose(
        jnp.concatenate([weight_ref[...], jnp.zeros((6, tokens), F32)], axis=0)
    )
    far_blocks = list(range(3, chips - 2)) if chips > 4 else [2]
    near = 2 if chips > 4 else 1
    firsts = [0] + far_blocks

    def fill(b, rel):
        t = wrapped(rel) * 2 + core
        columns = pl.ds(pl.multiple_of(t * LANE, LANE), LANE)
        cot = cot_ref[:, columns].astype(F32)
        ours = input_ref[:, columns]
        ins = mm(table[...], jnp.concatenate([ours, ours], axis=0))
        weighted = [(weights[:, j : j + 1] * cot).astype(BF) for j in (0, 1)]
        cots = mm(table[...], jnp.concatenate(weighted, axis=0))
        send[b, :, :capacity] = ins.astype(BF).reshape(groups, capacity, LANE)
        send[b, :, capacity:] = cots.astype(BF).reshape(groups, capacity, LANE)
        rows[t, sp] = send[b, sp]

    def dispatch(b, rel):
        t = wrapped(rel) * 2 + core

        @pl.loop(1, groups)
        def _(o):
            peer = lax.rem(sp + o, groups)
            to(send.at[b, peer], rows.at[t, sp], disp_s.at[b], disp_r.at[b], sp=peer)

    for copy in loads[2:5]:
        copy.wait()
    for copy in [*loads[5:], *copies]:
        copy.start()
    fill(0, 0)
    totals = mm(jnp.ones((8, tokens), F32), log_ref[...], NT, HIGH)
    tot_out[...] = jnp.concatenate(
        [totals, jnp.zeros((8, LANE - DK), F32)], axis=1
    )
    tot_in[sp] = tot_out[...]
    pl.semaphore_wait(barrier, groups - 1 + chips)

    dispatch(0, 0)
    for b, rel in enumerate(firsts):
        if b:
            fill(b, rel)
            dispatch(b, rel)

    @pl.loop(1, groups)
    def _(o):
        peer = lax.rem(sp + o, groups)
        to(tot_out, tot_in.at[sp], tot_s, tot_r, sp=peer)

    for copy in loads[5:]:
        copy.wait()

    @pl.loop(1, groups)
    def _(o):
        peer = lax.rem(sp + o, groups)
        to(saved_ref, all_saved.at[sp], save_s, save_r, sp=peer)

    all_saved[sp] = saved_ref[...]
    gu_acc[...] = jnp.zeros_like(gu_acc)
    hid_acc[...] = jnp.zeros_like(hid_acc)

    def halves(t, h):
        return rows.at[t, pl.ds(h * half, half)]

    def block(rel):
        return wrapped(rel) * 2 + core

    def pass_ring(rel, step, h, side):
        chip = wrapped(1 if side == 0 else chips - 1)
        part = halves(block(rel), h)
        to_tp(part, part, ring_s.at[step, side, h], ring_r.at[step, side, h], chip, core)

    def await_ring(rel, step, h, side):
        waited(halves(block(rel), h), ring_r.at[step, side, h])

    def to_other(rel):
        t = block(rel)
        to_tp(rows.at[t], rows.at[t], core_s.at[rel], core_r.at[rel], z, other)

    def from_other(rel):
        waited(rows.at[wrapped(rel) * 2 + other], core_r.at[rel])

    def both(zz, start):
        pieces = [
            rows[zz * 2 + k, :, start : start + capacity].reshape(slots, LANE) for k in (0, 1)
        ]
        return jnp.concatenate(pieces, axis=1)

    def gather_product(rel):
        zz = wrapped(rel)
        depth = pl.ds(pl.multiple_of(zz * 2 * LANE, 2 * LANE), 2 * LANE)
        ins = both(zz, 0)
        gu_acc[...] += mm(ins, wgu[depth, :])
        hid_acc[...] += mm(both(zz, capacity), wd[:, depth], NT)

    def await_dispatch(b):
        waited(send.at[b, pl.ds(0, groups - 1)], disp_r.at[b])

    def drain(phase):
        if phase >= 2:
            for b in range(len(firsts)):
                waited(send.at[b, pl.ds(0, groups - 1)], disp_s.at[b])
            waited(tot_in.at[pl.ds(0, groups - 1)], tot_s)
            waited(all_saved.at[pl.ds(0, groups - 1)], save_s)
        if phase >= 3:
            for step in range(near):
                for side in (0, 1):
                    for h in (0, 1):
                        waited(halves(0, h), ring_s.at[step, side, h])
            for rel in range(chips):
                waited(rows.at[0], core_s.at[rel])
        if phase >= 4:
            for j in range(chips):
                waited(pair_out.at[j], pair_s.at[j])
                if j < 2:
                    waited(near_out.at[j], near_s.at[j])
                else:
                    waited(back_out.at[j, pl.ds(0, groups - 1)], back_s.at[j])
                if 2 <= j < chips - 1:
                    waited(far_out.at[j], far_s.at[j])
        if phase >= 5:
            for rel in range(chips):
                waited(grad_in.at[0], fwd_s.at[rel])
                if rel not in (0, chips // 2):
                    waited(grad_in.at[0], all_s.at[rel])
            for side in (0, 1):
                waited(grad_in.at[0, pl.ds(0, tokens // 2)], opp_s.at[side])
        if phase >= 6:
            @pl.when(lax.rem(sp, 2) == core)
            def _():
                waited(all_in.at[pl.ds(0, chips - 1)], pj_s)
                waited(all_in, mate_s)

            @pl.when(lax.rem(sp, 2) != core)
            def _():
                waited(all_in.at[pl.ds(0, chips)], pj_s)

            for r in range(groups - 1):
                @pl.when(sp > r)
                def _():
                    waited(carry_out.at[r], carry_s.at[r])

    await_dispatch(0)
    for h in (0, 1):
        for side in (0, 1):
            pass_ring(0, 0, h, side)
    to_other(0)
    for copy in copies:
        copy.wait()
    from_other(0)
    gather_product(0)
    for h in (0, 1):
        for side in (0, 1):
            rel = chips - 1 if side == 0 else 1
            await_ring(rel, 0, h, side)
            if near > 1:
                pass_ring(rel, 1, h, side)
        if h == 0 and len(firsts) > 1:
            await_dispatch(1)
            to_other(firsts[1])
    to_other(1)
    to_other(chips - 1)
    for b, rel in enumerate(firsts):
        if b > 1:
            await_dispatch(b)
            to_other(rel)

    @pl.loop(0, len(far_blocks))
    def _(i):
        rel = far_blocks[0] + i
        from_other(rel)
        gather_product(rel)

    @pl.loop(0, 2)
    def _(i):
        rel = 1 + i * (chips - 2)
        from_other(rel)
        gather_product(rel)

    if near > 1:
        for side in (0, 1):
            rel = chips - 2 if side == 0 else 2
            for h in (0, 1):
                await_ring(rel, 1, h, side)
            to_other(rel)

        @pl.loop(0, 2)
        def _(i):
            rel = chips - 2 - i * (chips - 4)
            from_other(rel)
            gather_product(rel)

    tile = LANE

    @pl.loop(0, slots // tile)
    def _(i):
        at = pl.ds(pl.multiple_of(i * tile, tile), tile)
        gate = gu_acc[at, :hidden]
        upper = gu_acc[at, hidden:]
        d_hidden = hid_acc[at, :]
        sigmoid = jax.nn.sigmoid(gate)
        active = gate * sigmoid
        hid_t[:, at] = jnp.transpose(active * upper).astype(BF)
        dgu[at, hidden:] = (d_hidden * active).astype(BF)
        dgu[at, :hidden] = (
            d_hidden * upper * sigmoid * (1.0 + gate * (1.0 - sigmoid))
        ).astype(BF)

    def turn(j):
        far = chips // 2 + lax.div(j - 1, 2) * (2 * lax.rem(j, 2) - 1)
        rel = jnp.where(j < 2, 1 + j * (chips - 2), jnp.where(j == chips - 1, 0, far))
        return rel

    def slot_block(j):
        zz = wrapped(turn(j))
        depth = pl.ds(pl.multiple_of(zz * 2 * LANE, 2 * LANE), 2 * LANE)
        tmp[...] = mm(dgu[...], wgu[depth, :], NT)
        pair_out[j] = tmp[:, pl.ds(pl.multiple_of(other * LANE, LANE), LANE)].astype(BF)
        mine[j] = tmp[:, pl.ds(pl.multiple_of(core * LANE, LANE), LANE)]
        to_tp(pair_out.at[j], pair_in.at[j], pair_s.at[j], pair_r.at[j], z, other)

    def slot_near(j):
        waited(pair_in.at[j], pair_r.at[j])
        near_out[j] = (mine[j] + pair_in[j].astype(F32)).astype(BF)
        to_tp(
            near_out.at[j], near_in.at[j], near_s.at[j], near_r.at[j], wrapped(turn(j)), core
        )

    def slot_send(j, whole):
        back_out[j] = whole.astype(BF).reshape(groups, capacity, LANE)
        back_in[j, sp] = back_out[j, sp]

        @pl.loop(1, groups)
        def _(o):
            peer = lax.rem(sp + o, groups)
            to(back_out.at[j, peer], back_in.at[j, sp], back_s.at[j], back_r.at[j], sp=peer)

    def slot_return(j):
        waited(pair_in.at[j], pair_r.at[j])
        slot_send(j, mine[j] + pair_in[j].astype(F32))

    lag = 2

    @pl.loop(0, chips + lag - 1)
    def _(j):
        @pl.when(j < chips)
        def _():
            slot_block(j)

        @pl.when((j >= lag) & (j < 2 * lag))
        def _():
            slot_near(j - lag)

        @pl.when(j >= 2 * lag)
        def _():
            slot_return(j - lag)

    def weight_block(zz):
        depth = pl.ds(pl.multiple_of(zz * 2 * LANE, 2 * LANE), 2 * LANE)
        pair = mm(both(zz, 0), dgu[...], TN).astype(BF)
        gg_ref[depth, :] = pair[:, :hidden]
        gu_ref[depth, :] = pair[:, hidden:]
        gw_ref[:, depth] = mm(hid_t[...], both(zz, capacity)).astype(BF)

    weight_block(0)
    weight_block(1)
    own = chips - 1
    waited(pair_in.at[own], pair_r.at[own])
    summed = mine[own] + pair_in[own].astype(F32)
    for j in (0, 1):
        waited(near_in.at[j], near_r.at[j])
        summed += near_in[j].astype(F32)
    slot_send(own, summed)

    def routed(j):
        waited(back_out.at[j, pl.ds(0, groups - 1)], back_r.at[j])
        return mm(picks[...], back_in[j].reshape(slots, LANE))

    @pl.loop(2, chips - 1)
    def _(j):
        rel = turn(j)
        far_out[j] = routed(j).astype(BF)
        to_tp(far_out.at[j], far_in.at[rel], far_s.at[j], far_r.at[rel], wrapped(rel), core)
        weight_block(j)

    weight_block(chips - 1)
    total = routed(chips - 1)
    same_span = lax.div(row, SPAN) == lax.div(col, SPAN)
    causal = (row >= col) & same_span
    until = ((row <= col) & same_span).astype(F32)
    since = causal.astype(F32)
    cum = mm(log_ref[...], until, NN, HIGH)
    waited(tot_in.at[pl.ds(0, groups - 1)], tot_r)
    after_row = lax.broadcasted_iota(jnp.int32, (groups, LANE), 0)
    after_col = lax.broadcasted_iota(jnp.int32, (groups, LANE), 1)
    between = ((after_row > after_col) & (after_row < sp)).astype(F32)
    factors = jnp.exp(mm(tot_in[:, 0, :DK], between, TN, HIGH))

    for rel in range(2, chips - 1):
        waited(far_in.at[rel], far_r.at[rel])
        total += far_in[rel].astype(F32)
    columns = pl.ds(pl.multiple_of(tp * LANE, LANE), LANE)
    grad_in[tp] = (cot_ref[:, columns].astype(F32) + total).astype(BF)
    reach = chips // 2 - 1
    order = [r for k in range(reach, 0, -1) for r in (k, chips - k)]
    for rel in order:
        to_tp(grad_in.at[tp], grad_in.at[tp], all_s.at[rel], all_r.at[rel], wrapped(rel), core)
    to_tp(grad_in.at[tp], grad_in.at[tp], fwd_s.at[0], fwd_r.at[0], z, other)

    def to_owner(t):
        @pl.when(t != sp)
        def _():
            to(grad_in.at[t], all_in.at[sp], pj_s, pj_r, sp=t)

        @pl.when(t == sp)
        def _():
            all_in[sp] = grad_in[t]

    def to_pair(rel, t):
        to_tp(grad_in.at[t], grad_in.at[t], fwd_s.at[rel], fwd_r.at[rel], z, other)

    half_rows = tokens // 2
    to_owner(tp)
    for rel in order:
        t = wrapped(chips - rel) * 2 + core
        waited(grad_in.at[t], all_r.at[rel])
        if rel in (reach, chips - reach):
            side = 0 if rel == reach else 1
            part = grad_in.at[t, pl.ds(side * half_rows, half_rows)]
            chip = wrapped(1 if side == 0 else chips - 1)
            to_tp(part, part, opp_s.at[side], opp_r.at[side], chip, core)
        to_pair(rel, t)
        to_owner(t)
    t = wrapped(chips // 2) * 2 + core
    for side in (0, 1):
        waited(grad_in.at[t, pl.ds(0, half_rows)], opp_r.at[side])
    to_pair(chips // 2, t)
    to_owner(t)
    for rel in [0, *order, chips // 2]:
        t = wrapped(chips - rel if rel else 0) * 2 + other
        waited(grad_in.at[t], fwd_r.at[rel])

    mix = jnp.zeros((tokens, LANE), F32)
    for zz in range(chips):
        pair = jnp.concatenate([grad_in[2 * zz], grad_in[2 * zz + 1]], axis=1)
        mix += mm(pair, proj_ref[:, 2 * zz * LANE : 2 * (zz + 1) * LANE], NT)

    scale = DK ** (-0.5)
    grown = jnp.exp(cum)
    shrunk = jnp.exp(-cum)
    queries = q_ref[...].astype(F32)
    keys = k_ref[...].astype(F32)
    qd = (queries * grown).astype(BF)
    kd = (keys * shrunk).astype(BF)
    mix_half = mix.astype(BF)
    spans = [slice(n * SPAN, (n + 1) * SPAN) for n in (0, 1)]
    local = [scale * mm(qd[:, s], mix_half[s]) for s in spans]
    ends = [cum[:, (n + 1) * SPAN - 1 : (n + 1) * SPAN] for n in (0, 1)]
    last = [jnp.exp(e) for e in ends]
    begin = local[0] + last[0] * local[1]
    for r in range(groups - 1):
        @pl.when(sp > r)
        def _():
            carry_out[r] = (begin * factors[:, r : r + 1]).astype(BF)
            to(carry_out.at[r], carry_in.at[sp], carry_s.at[r], carry_r.at[sp], sp=r)

    values = v_ref[...]
    to_end = jnp.concatenate([jnp.exp(ends[n] - cum[:, spans[n]]) for n in (0, 1)], axis=1)
    ke = (keys * to_end).astype(BF)
    scores = jnp.where(causal, mm(qd, kd, TN), 0.0).astype(BF)
    dots = jnp.where(causal, mm(mix_half, values, NT), 0.0).astype(BF)
    from_state = jnp.concatenate(
        [mm(state_ref[n].astype(BF), mix_half[spans[n]], NT) for n in (0, 1)], axis=1
    )
    dq = scale * grown * (mm(kd, dots, NT) + from_state)
    dk = scale * shrunk * mm(qd, dots)
    dv = scale * mm(scores, mix_half, TN)
    state_end = [last[n] * state_ref[n] + mm(ke[:, spans[n]], values[spans[n]]) for n in (0, 1)]
    gq_ref[...] = dq.astype(BF)

    mate = lax.rem(sp, 2) == core

    @pl.when(mate)
    def _():
        waited(all_in.at[pl.ds(0, groups - 1)], pj_r)
        to_tp(all_in, all_in, mate_s, mate_r, z, other)

    after[...] = jnp.zeros_like(after)
    for s in range(1, groups):
        @pl.when(s > sp)
        def _():
            waited(carry_in.at[s], carry_r.at[s])
            after[...] += carry_in[s].astype(F32)

    end_1 = after[...]
    g_end = [local[1] + last[1] * end_1, end_1]
    half_end = [g.astype(BF) for g in g_end]
    dk = dk + to_end * jnp.concatenate(
        [mm(half_end[n], values[spans[n]], NT) for n in (0, 1)], axis=1
    )
    dv = dv + jnp.concatenate([mm(ke[:, spans[n]], half_end[n], TN) for n in (0, 1)], axis=0)
    tails = [jnp.sum(state_end[n] * g_end[n], axis=1, keepdims=True) for n in (0, 1)]
    tail = jnp.concatenate([jnp.broadcast_to(t, (DK, SPAN)) for t in tails], axis=1)
    gd_ref[...] = mm(queries * dq - keys * dk, since, NN, HIGH) + tail
    gk_ref[...] = dk.astype(BF)
    gv_ref[...] = dv.astype(BF)

    @pl.when(jnp.logical_not(mate))
    def _():
        waited(all_in, mate_r)

    waited(all_saved.at[pl.ds(0, groups - 1)], save_r)
    depth = groups * tokens
    gproj_ref[...] = mm(
        all_in[...].reshape(depth, LANE), all_saved[...].reshape(depth, LANE), TN
    )
    drain(6)


def store_kernel(*refs):
    count = (len(refs) - 1) // 2
    sems = refs[-1]
    copies = []
    for n, (src, dst) in enumerate(zip(refs[:count], refs[count : 2 * count])):
        copy = pltpu.make_async_copy(src, dst.at[0] if len(dst.shape) > 2 else dst, sems.at[n])
        copy.start()
        copies.append(copy)
    for copy in copies:
        copy.wait()


def on_device(
    moe_input, cotangent, route_expert, route_weight, w_gate, w_up, w_down, out_proj, saved_out,
    queries, keys, values, log_decay, span_state,
):
    groups, lanes = lax.axis_size("sp"), lax.axis_size("tp")
    tokens, width = moe_input.shape
    capacity = 4 * tokens // groups
    slots = groups * capacity
    hidden = w_gate.shape[2]
    chips = lanes // 2
    firsts = 4 if chips > 4 else 2
    vmem = pl.BlockSpec(memory_space=pltpu.VMEM)
    hbm = pl.BlockSpec(memory_space=pltpu.HBM)
    dma = pltpu.SemaphoreType.DMA
    shape = jax.ShapeDtypeStruct
    slab = (groups, 2 * capacity, LANE)
    scratch = [
        pltpu.VMEM((2, tokens), jnp.int32),
        pltpu.VMEM((2, tokens), F32),
        pltpu.VMEM((tokens, width), BF),
        pltpu.VMEM((tokens, width), BF),
        pltpu.VMEM((LANE, width), BF),
        pltpu.VMEM((tokens, LANE), BF),
        pltpu.VMEM((DK, tokens), BF),
        pltpu.VMEM((DK, tokens), BF),
        pltpu.VMEM((tokens, LANE), BF),
        pltpu.VMEM((DK, tokens), F32),
        pltpu.VMEM((2, DK, LANE), F32),
        pltpu.VMEM((width, 2 * hidden), BF),
        pltpu.VMEM((hidden, width), BF),
        pltpu.VMEM((lanes, *slab), BF),
        pltpu.VMEM((hidden, slots), BF),
        pltpu.VMEM((slots, 2 * hidden), BF),
        pltpu.VMEM((slots, 2 * tokens), BF),
        pltpu.VMEM((tokens, slots), BF),
        pltpu.VMEM((firsts, *slab), BF),
        pltpu.VMEM((slots, 2 * hidden), F32),
        pltpu.VMEM((slots, hidden), F32),
        pltpu.VMEM((slots, 2 * LANE), F32),
        pltpu.VMEM((chips, slots, LANE), F32),
        pltpu.VMEM((chips, slots, LANE), BF),
        pltpu.VMEM((chips, slots, LANE), BF),
        pltpu.VMEM((2, slots, LANE), BF),
        pltpu.VMEM((2, slots, LANE), BF),
        pltpu.VMEM((chips, groups, capacity, LANE), BF),
        pltpu.VMEM((chips, groups, capacity, LANE), BF),
        pltpu.VMEM((chips, tokens, LANE), BF),
        pltpu.VMEM((chips, tokens, LANE), BF),
        pltpu.VMEM((lanes, tokens, LANE), BF),
        pltpu.VMEM((groups, tokens, LANE), BF),
        pltpu.VMEM((groups, tokens, LANE), BF),
        pltpu.VMEM((8, LANE), F32),
        pltpu.VMEM((groups, 8, LANE), F32),
        pltpu.VMEM((groups, DK, LANE), BF),
        pltpu.VMEM((groups, DK, LANE), BF),
        pltpu.VMEM((DK, LANE), F32),
        dma((3,)), dma((11,)),
        dma((firsts,)), dma((firsts,)),
        dma((2, 2, 2)), dma((2, 2, 2)),
        dma((chips,)), dma((chips,)),
        dma((chips,)), dma((chips,)),
        dma((2,)), dma((2,)),
        dma((chips,)), dma((chips,)),
        dma((chips,)), dma((chips,)),
        dma((chips,)), dma((chips,)),
        dma((chips,)), dma((chips,)),
        dma, dma, dma((2,)), dma((2,)), dma, dma,
        dma, dma, dma, dma,
        dma((groups,)), dma((groups,)),
    ]
    made = (
        pltpu.VMEM((width, hidden), BF),
        pltpu.VMEM((width, hidden), BF),
        pltpu.VMEM((hidden, width), BF),
        pltpu.VMEM((LANE, LANE), F32),
        pltpu.VMEM((DK, tokens), BF),
        pltpu.VMEM((DK, tokens), BF),
        pltpu.VMEM((tokens, LANE), BF),
        pltpu.VMEM((DK, tokens), F32),
    )
    results = pl.pallas_call(
        functools.partial(main_kernel, groups=groups, lanes=lanes, capacity=capacity),
        name="experts_and_attention",
        out_shape=made,
        in_specs=[hbm] * 14,
        out_specs=(vmem,) * 8,
        scratch_shapes=scratch,
        compiler_params=pltpu.CompilerParams(
            collective_id=0, has_side_effects=True, vmem_limit_bytes=62105600
        ),
    )(
        route_expert.T, route_weight.T, moe_input, cotangent, out_proj, saved_out, queries.T,
        keys.T, values, log_decay.T, span_state, w_gate, w_up, w_down,
    )
    results = pl.pallas_call(
        store_kernel,
        name="store_results",
        out_shape=tuple(
            shape((1, *a.shape) if n < 3 else a.shape, a.dtype) for n, a in enumerate(results)
        ),
        in_specs=[vmem] * 8,
        out_specs=(hbm,) * 8,
        scratch_shapes=[dma((8,))],
        compiler_params=pltpu.CompilerParams(vmem_limit_bytes=1024 * 1024),
    )(*(pltpu.with_memory_space_constraint(r, pltpu.VMEM) for r in results))
    gg, gu, gw, gp, gq, gk, gv, gd = results
    return gg, gu, gw, gp, gq.T, gk.T, gv, gd.T


def solution(mesh):
    placed = (
        P("sp", None),
        P("sp", None),
        P("sp", None),
        P("sp", None),
        P("sp", None, "tp"),
        P("sp", None, "tp"),
        P("sp", "tp", None),
        P("tp", None),
        P("sp", "tp"),
        P("sp", "tp"),
        P("sp", "tp"),
        P("sp", "tp"),
        P("sp", "tp"),
        P("sp", "tp", None),
    )
    return jax.shard_map(
        on_device,
        mesh=mesh,
        in_specs=placed,
        out_specs=(
            P("sp", None, "tp"),
            P("sp", None, "tp"),
            P("sp", "tp", None),
            P("sp", "tp"),
            P("sp", "tp"),
            P("sp", "tp"),
            P("sp", "tp"),
            P("sp", "tp"),
        ),
        check_vma=False,
    )
```

```python
import functools

import jax
import jax.numpy as jnp
from jax import lax
from jax.experimental import pallas as pl
from jax.experimental.pallas import tpu as pltpu
from jax.sharding import PartitionSpec as P

BF = jnp.bfloat16
F32 = jnp.float32
HIGH = lax.Precision.HIGHEST
LANE = 128
DK = 64
SPAN = 64
NN = (((1,), (0,)), ((), ()))
NT = (((1,), (1,)), ((), ()))
TN = (((0,), (0,)), ((), ()))


def mm(a, b, dims=NN, precision=None):
    return lax.dot_general(a, b, dims, precision=precision, preferred_element_type=F32)


def half_dot(a, b, dims=NN):
    return mm(a.astype(BF), b.astype(BF), dims)


def waited(ref, sem):
    pltpu.make_async_copy(ref, ref, sem).wait()


def main_kernel(
    route_hbm, weight_hbm, input_hbm, cot_hbm, proj_hbm, saved_hbm, q_hbm, k_hbm, v_hbm, log_hbm,
    state_hbm, wg_hbm, wu_hbm, wd_hbm,
    gg_ref, gu_ref, gw_ref, gproj_ref, gq_ref, gk_ref, gv_ref, gd_ref,
    route_ref, weight_ref, input_ref, cot_ref, proj_ref, saved_ref, q_ref, k_ref, v_ref, log_ref,
    state_ref, wgu, wd, rows, hid_t, dgu, table, picks, send, gu_acc, hid_acc, tmp, mine, pair_out,
    pair_in, near_out, near_in, back_out, back_in, far_out, far_in, grad_in, all_in, all_saved,
    tot_out, tot_in,
    carry_out, carry_in, after,
    w_sem, load_sem, disp_s, disp_r, ring_s, ring_r, core_s, core_r, late_s, late_r, pair_s, pair_r, near_s, near_r, back_s, back_r,
    far_s, far_r, all_s, all_r, fwd_s, fwd_r, save_s, save_r, opp_s, opp_r, mate_s, mate_r, pj_s, pj_r, tot_s, tot_r, carry_s, carry_r,
    *, groups, lanes, capacity,
):
    chips = lanes // 2
    sp, tp = lax.axis_index("sp"), lax.axis_index("tp")
    z, core = lax.div(tp, 2), lax.rem(tp, 2)
    other = 1 - core
    tokens = input_ref.shape[0]
    slots = groups * capacity
    hidden = wd.shape[0]

    def wrapped(rel):
        return lax.rem(z + rel, chips)

    def to(src, dst, send_sem, recv_sem, **where):
        pltpu.make_async_remote_copy(
            src_ref=src, dst_ref=dst, send_sem=send_sem, recv_sem=recv_sem,
            device_id=where, device_id_type=pl.DeviceIdType.MESH,
        ).start()

    def to_tp(src, dst, send_sem, recv_sem, chip, at_core):
        to(src, dst, send_sem, recv_sem, tp=chip * 2 + at_core)

    barrier = pltpu.get_barrier_semaphore()

    @pl.loop(1, groups)
    def _(o):
        pl.semaphore_signal(
            barrier, inc=1, device_id={"sp": lax.rem(sp + o, groups)},
            device_id_type=pl.DeviceIdType.MESH,
        )

    @pl.loop(1, chips)
    def _(o):
        pl.semaphore_signal(
            barrier, inc=1, device_id={"tp": wrapped(o) * 2 + core},
            device_id_type=pl.DeviceIdType.MESH,
        )

    pl.semaphore_signal(
        barrier, inc=1, device_id={"tp": z * 2 + other}, device_id_type=pl.DeviceIdType.MESH
    )

    given = [
        route_hbm, weight_hbm, input_hbm, cot_hbm, log_hbm, proj_hbm, saved_hbm, q_hbm, k_hbm,
        v_hbm, state_hbm,
    ]
    held = [
        route_ref, weight_ref, input_ref, cot_ref, log_ref, proj_ref, saved_ref, q_ref, k_ref,
        v_ref, state_ref,
    ]
    loads = [
        pltpu.make_async_copy(src, dst, load_sem.at[n])
        for n, (src, dst) in enumerate(zip(given, held))
    ]
    for copy in loads[:5]:
        copy.start()
    copies = [
        pltpu.make_async_copy(wg_hbm.at[0], wgu.at[:, pl.ds(0, hidden)], w_sem.at[0]),
        pltpu.make_async_copy(wu_hbm.at[0], wgu.at[:, pl.ds(hidden, hidden)], w_sem.at[1]),
        pltpu.make_async_copy(wd_hbm.at[0], wd, w_sem.at[2]),
    ]
    for copy in loads[:2]:
        copy.wait()
    experts = lax.broadcasted_iota(jnp.int32, (groups, tokens), 0)
    named = [(route_ref[j : j + 1, :] == experts).astype(F32) for j in (0, 1)]
    row = lax.broadcasted_iota(jnp.int32, (tokens, tokens), 0)
    col = lax.broadcasted_iota(jnp.int32, (tokens, tokens), 1)
    earlier = half_dot(named[0] + named[1], (row < col).astype(F32))
    place_in = lax.broadcasted_iota(jnp.int32, (slots, tokens), 0)
    found = []
    for j in (0, 1):
        place = jnp.sum(earlier * named[j], axis=0, keepdims=True).astype(jnp.int32)
        slot = route_ref[j : j + 1, :] * capacity + place
        found.append((slot == place_in).astype(F32))
        table[:, j * tokens : (j + 1) * tokens] = found[j].astype(BF)
    picks[...] = jnp.transpose(found[0] + found[1]).astype(BF)
    weights = jnp.transpose(
        jnp.concatenate([weight_ref[...], jnp.zeros((6, tokens), F32)], axis=0)
    )
    far_blocks = range(3, chips - 2)
    late = (2, chips - 2)
    firsts = [0, *far_blocks, *late]

    def fill(b, rel):
        t = wrapped(rel) * 2 + core
        columns = pl.ds(pl.multiple_of(t * LANE, LANE), LANE)
        if rel not in late:
            ours = input_ref[:, columns]
            ins = mm(table[...], jnp.concatenate([ours, ours], axis=0))
            send[b, 0] = ins.astype(BF).reshape(groups, capacity, LANE)
            rows[t, 0, sp] = send[b, 0, sp]
        cot = cot_ref[:, columns].astype(F32)
        weighted = [(weights[:, j : j + 1] * cot).astype(BF) for j in (0, 1)]
        cots = mm(table[...], jnp.concatenate(weighted, axis=0))
        send[b, 1] = cots.astype(BF).reshape(groups, capacity, LANE)
        rows[t, 1, sp] = send[b, 1, sp]

    def dispatch(b, rel, p):
        t = wrapped(rel) * 2 + core

        @pl.loop(1, groups)
        def _(o):
            peer = lax.rem(sp + o, groups)
            to(send.at[b, p, peer], rows.at[t, p, sp], disp_s.at[b, p], disp_r.at[b, p], sp=peer)

    def pieces(rel):
        return (1,) if rel in late else (0, 1)

    for copy in loads[2:5]:
        copy.wait()
    for copy in [*loads[5:], *copies]:
        copy.start()
    fill(0, 0)
    totals = mm(jnp.ones((8, tokens), F32), log_ref[...], NT, HIGH)
    tot_out[...] = jnp.concatenate(
        [totals, jnp.zeros((8, LANE - DK), F32)], axis=1
    )
    tot_in[sp] = tot_out[...]
    pl.semaphore_wait(barrier, groups - 1 + chips)

    for b, rel in enumerate(firsts):
        if b:
            fill(b, rel)
        for p in pieces(rel):
            dispatch(b, rel, p)

    @pl.loop(1, groups)
    def _(o):
        peer = lax.rem(sp + o, groups)
        to(tot_out, tot_in.at[sp], tot_s, tot_r, sp=peer)

    for copy in loads[5:]:
        copy.wait()
    gu_acc[...] = jnp.zeros_like(gu_acc)
    hid_acc[...] = jnp.zeros_like(hid_acc)

    def block(rel):
        return wrapped(rel) * 2 + core

    def pass_ring(rel, step, p, side):
        chip = wrapped(1 if side == 0 else chips - 1)
        part = rows.at[block(rel), p]
        to_tp(part, part, ring_s.at[step, side, p], ring_r.at[step, side, p], chip, core)

    def await_ring(rel, step, p, side):
        waited(rows.at[block(rel), p], ring_r.at[step, side, p])

    def to_other(rel):
        t = block(rel)
        to_tp(rows.at[t], rows.at[t], core_s.at[rel], core_r.at[rel], z, other)

    def from_other(rel):
        waited(rows.at[wrapped(rel) * 2 + other], core_r.at[rel])

    def late_to_other(i, p):
        part = rows.at[block(late[i]), p]
        to_tp(part, part, late_s.at[i, p], late_r.at[i, p], z, other)

    def both(zz, p):
        return jnp.concatenate(
            [rows[zz * 2 + k, p].reshape(slots, LANE) for k in (0, 1)], axis=1
        )

    def depth_of(zz):
        return pl.ds(pl.multiple_of(zz * 2 * LANE, 2 * LANE), 2 * LANE)

    def gather_product(rel):
        zz = wrapped(rel)
        gu_acc[...] += mm(both(zz, 0), wgu[depth_of(zz), :])
        hid_acc[...] += mm(both(zz, 1), wd[:, depth_of(zz)], NT)

    def await_dispatch(b, p):
        waited(send.at[b, p, pl.ds(0, groups - 1)], disp_r.at[b, p])

    def drain(phase):
        if phase >= 2:
            for b, rel in enumerate(firsts):
                for p in pieces(rel):
                    waited(send.at[b, p, pl.ds(0, groups - 1)], disp_s.at[b, p])
            waited(tot_in.at[pl.ds(0, groups - 1)], tot_s)
        if phase >= 3:
            for side in (0, 1):
                waited(rows.at[0, 0], ring_s.at[0, side, 0])
                waited(rows.at[0, 0], ring_s.at[0, side, 1])
                waited(rows.at[0, 0], ring_s.at[1, side, 0])
                for p in (0, 1):
                    waited(rows.at[0, 0], late_s.at[side, p])
            for rel in range(chips):
                if rel not in late:
                    waited(rows.at[0], core_s.at[rel])
        if phase >= 4:
            waited(all_saved.at[pl.ds(0, groups - 1)], save_s)
            for j in range(chips):
                waited(pair_out.at[j], pair_s.at[j])
                if j in (2, 3):
                    waited(near_out.at[j - 2], near_s.at[j - 2])
                else:
                    waited(back_out.at[j, pl.ds(0, groups - 1)], back_s.at[j])
                    if j < chips - 1:
                        waited(far_out.at[j], far_s.at[j])
        if phase >= 5:
            for rel in range(chips):
                waited(grad_in.at[0], fwd_s.at[rel])
                if rel not in (0, chips // 2):
                    waited(grad_in.at[0], all_s.at[rel])
            for side in (0, 1):
                waited(grad_in.at[0, pl.ds(0, tokens // 2)], opp_s.at[side])
        if phase >= 6:
            @pl.when(lax.rem(sp, 2) == core)
            def _():
                waited(all_in.at[pl.ds(0, chips - 1)], pj_s)
                waited(all_in, mate_s)

            @pl.when(lax.rem(sp, 2) != core)
            def _():
                waited(all_in.at[pl.ds(0, chips)], pj_s)

            for r in range(groups - 1):
                @pl.when(sp > r)
                def _():
                    waited(carry_out.at[r], carry_s.at[r])

    for p in (0, 1):
        await_dispatch(0, p)
        for side in (0, 1):
            pass_ring(0, 0, p, side)
    to_other(0)
    for copy in copies:
        copy.wait()
    from_other(0)
    gather_product(0)
    for side in (0, 1):
        rel = chips - 1 if side == 0 else 1
        await_ring(rel, 0, 0, side)
        pass_ring(rel, 1, 0, side)
    for p in (0, 1):
        await_dispatch(1, p)
    to_other(firsts[1])
    for side in (0, 1):
        rel = chips - 1 if side == 0 else 1
        await_ring(rel, 0, 1, side)
        to_other(rel)
    for p in (0, 1):
        await_dispatch(2, p)
    to_other(firsts[2])

    @pl.loop(0, 2)
    def _(i):
        rel = 1 + i * (chips - 2)
        from_other(rel)
        gather_product(rel)

    for p in (0, 1):
        await_dispatch(3, p)
    to_other(firsts[3])

    @pl.loop(0, len(far_blocks) - 1)
    def _(i):
        rel = far_blocks[0] + i
        from_other(rel)
        gather_product(rel)

    for i in (0, 1):
        await_ring(late[i], 1, 0, 1 - i)
        late_to_other(i, 0)
    from_other(far_blocks[-1])
    gather_product(far_blocks[-1])
    for i in (0, 1):
        await_dispatch(4 + i, 1)
        late_to_other(i, 1)
    for p in (0, 1):
        for i in (0, 1):
            zz = wrapped(late[i])
            waited(rows.at[zz * 2 + other, p], late_r.at[i, p])
            if p == 0:
                gu_acc[...] += mm(both(zz, 0), wgu[depth_of(zz), :])
            else:
                hid_acc[...] += mm(both(zz, 1), wd[:, depth_of(zz)], NT)

    tile = LANE

    @pl.loop(0, slots // tile)
    def _(i):
        at = pl.ds(pl.multiple_of(i * tile, tile), tile)
        gate = gu_acc[at, :hidden]
        upper = gu_acc[at, hidden:]
        d_hidden = hid_acc[at, :]
        sigmoid = jax.nn.sigmoid(gate)
        active = gate * sigmoid
        hid_t[:, at] = jnp.transpose(active * upper).astype(BF)
        dgu[at, hidden:] = (d_hidden * active).astype(BF)
        dgu[at, :hidden] = (
            d_hidden * upper * sigmoid * (1.0 + gate * (1.0 - sigmoid))
        ).astype(BF)

    def turn(j):
        k = jnp.where(j < 2, j, j - 2)
        far = chips // 2 + lax.div(k + 1, 2) * (2 * lax.rem(k, 2) - 1)
        near = 1 + (j - 2) * (chips - 2)
        return jnp.where((j == 2) | (j == 3), near, jnp.where(j == chips - 1, 0, far))

    def slot_block(j):
        zz = wrapped(turn(j))
        depth = pl.ds(pl.multiple_of(zz * 2 * LANE, 2 * LANE), 2 * LANE)
        tmp[...] = mm(dgu[...], wgu[depth, :], NT)
        pair_out[j] = tmp[:, pl.ds(pl.multiple_of(other * LANE, LANE), LANE)].astype(BF)
        mine[j] = tmp[:, pl.ds(pl.multiple_of(core * LANE, LANE), LANE)]
        to_tp(pair_out.at[j], pair_in.at[j], pair_s.at[j], pair_r.at[j], z, other)

    def slot_near(j):
        waited(pair_in.at[j], pair_r.at[j])
        side = j - 2
        near_out[side] = (mine[j] + pair_in[j].astype(F32)).astype(BF)
        to_tp(
            near_out.at[side], near_in.at[side], near_s.at[side], near_r.at[side],
            wrapped(turn(j)), core,
        )

    def slot_send(j, whole):
        back_out[j] = whole.astype(BF).reshape(groups, capacity, LANE)
        back_in[j, sp] = back_out[j, sp]

        @pl.loop(1, groups)
        def _(o):
            peer = lax.rem(sp + o, groups)
            to(back_out.at[j, peer], back_in.at[j, sp], back_s.at[j], back_r.at[j], sp=peer)

    def slot_return(j):
        waited(pair_in.at[j], pair_r.at[j])
        slot_send(j, mine[j] + pair_in[j].astype(F32))

    lag = 2

    @pl.loop(0, chips + lag - 1)
    def _(j):
        @pl.when(j < chips)
        def _():
            slot_block(j)

        i = j - lag

        @pl.when((i == 2) | (i == 3))
        def _():
            slot_near(i)

        @pl.when((i >= 0) & (i != 2) & (i != 3))
        def _():
            slot_return(i)

    def weight_block(zz):
        depth = depth_of(zz)
        pair = mm(both(zz, 0), dgu[...], TN).astype(BF)
        gg_ref[depth, :] = pair[:, :hidden]
        gu_ref[depth, :] = pair[:, hidden:]
        gw_ref[:, depth] = mm(hid_t[...], both(zz, 1)).astype(BF)

    weight_block(0)
    weight_block(1)
    own = chips - 1
    waited(pair_in.at[own], pair_r.at[own])
    summed = mine[own] + pair_in[own].astype(F32)
    for j in (0, 1):
        waited(near_in.at[j], near_r.at[j])
        summed += near_in[j].astype(F32)
    slot_send(own, summed)

    @pl.loop(1, groups)
    def _(o):
        peer = lax.rem(sp + o, groups)
        to(saved_ref, all_saved.at[sp], save_s, save_r, sp=peer)

    all_saved[sp] = saved_ref[...]

    def routed(j):
        waited(back_out.at[j, pl.ds(0, groups - 1)], back_r.at[j])
        return mm(picks[...], back_in[j].reshape(slots, LANE))

    @pl.loop(0, chips - 3)
    def _(i):
        j = jnp.where(i < 2, i, i + 2)
        rel = turn(j)
        far_out[j] = routed(j).astype(BF)
        to_tp(far_out.at[j], far_in.at[rel], far_s.at[j], far_r.at[rel], wrapped(rel), core)
        weight_block(i + 2)

    weight_block(chips - 1)
    total = routed(chips - 1)
    same_span = lax.div(row, SPAN) == lax.div(col, SPAN)
    causal = (row >= col) & same_span
    until = ((row <= col) & same_span).astype(F32)
    since = causal.astype(F32)
    cum = mm(log_ref[...], until, NN, HIGH)
    waited(tot_in.at[pl.ds(0, groups - 1)], tot_r)
    after_row = lax.broadcasted_iota(jnp.int32, (groups, LANE), 0)
    after_col = lax.broadcasted_iota(jnp.int32, (groups, LANE), 1)
    between = ((after_row > after_col) & (after_row < sp)).astype(F32)
    factors = jnp.exp(mm(tot_in[:, 0, :DK], between, TN, HIGH))

    for rel in range(2, chips - 1):
        waited(far_in.at[rel], far_r.at[rel])
        total += far_in[rel].astype(F32)
    columns = pl.ds(pl.multiple_of(tp * LANE, LANE), LANE)
    grad_in[tp] = (cot_ref[:, columns].astype(F32) + total).astype(BF)
    reach = chips // 2 - 1
    order = [r for k in range(reach, 0, -1) for r in (k, chips - k)]
    for rel in order:
        to_tp(grad_in.at[tp], grad_in.at[tp], all_s.at[rel], all_r.at[rel], wrapped(rel), core)
    to_tp(grad_in.at[tp], grad_in.at[tp], fwd_s.at[0], fwd_r.at[0], z, other)

    def to_owner(t):
        @pl.when(t != sp)
        def _():
            to(grad_in.at[t], all_in.at[sp], pj_s, pj_r, sp=t)

        @pl.when(t == sp)
        def _():
            all_in[sp] = grad_in[t]

    def to_pair(rel, t):
        to_tp(grad_in.at[t], grad_in.at[t], fwd_s.at[rel], fwd_r.at[rel], z, other)

    half_rows = tokens // 2
    to_owner(tp)
    for rel in order:
        t = wrapped(chips - rel) * 2 + core
        waited(grad_in.at[t], all_r.at[rel])
        if rel in (reach, chips - reach):
            side = 0 if rel == reach else 1
            part = grad_in.at[t, pl.ds(side * half_rows, half_rows)]
            chip = wrapped(1 if side == 0 else chips - 1)
            to_tp(part, part, opp_s.at[side], opp_r.at[side], chip, core)
        to_pair(rel, t)
        to_owner(t)
    t = wrapped(chips // 2) * 2 + core
    for side in (0, 1):
        waited(grad_in.at[t, pl.ds(0, half_rows)], opp_r.at[side])
    to_pair(chips // 2, t)
    to_owner(t)
    for rel in [0, *order, chips // 2]:
        t = wrapped(chips - rel if rel else 0) * 2 + other
        waited(grad_in.at[t], fwd_r.at[rel])

    mix = jnp.zeros((tokens, LANE), F32)
    for zz in range(chips):
        pair = jnp.concatenate([grad_in[2 * zz], grad_in[2 * zz + 1]], axis=1)
        mix += mm(pair, proj_ref[:, 2 * zz * LANE : 2 * (zz + 1) * LANE], NT)

    scale = DK ** (-0.5)
    grown = jnp.exp(cum)
    shrunk = jnp.exp(-cum)
    queries = q_ref[...].astype(F32)
    keys = k_ref[...].astype(F32)
    qd = (queries * grown).astype(BF)
    kd = (keys * shrunk).astype(BF)
    mix_half = mix.astype(BF)
    spans = [slice(n * SPAN, (n + 1) * SPAN) for n in (0, 1)]
    local = [scale * mm(qd[:, s], mix_half[s]) for s in spans]
    ends = [cum[:, (n + 1) * SPAN - 1 : (n + 1) * SPAN] for n in (0, 1)]
    last = [jnp.exp(e) for e in ends]
    begin = local[0] + last[0] * local[1]
    for r in range(groups - 1):
        @pl.when(sp > r)
        def _():
            carry_out[r] = (begin * factors[:, r : r + 1]).astype(BF)
            to(carry_out.at[r], carry_in.at[sp], carry_s.at[r], carry_r.at[sp], sp=r)

    values = v_ref[...]
    to_end = jnp.concatenate([jnp.exp(ends[n] - cum[:, spans[n]]) for n in (0, 1)], axis=1)
    ke = (keys * to_end).astype(BF)
    scores = jnp.where(causal, mm(qd, kd, TN), 0.0).astype(BF)
    dots = jnp.where(causal, mm(mix_half, values, NT), 0.0).astype(BF)
    from_state = jnp.concatenate(
        [mm(state_ref[n].astype(BF), mix_half[spans[n]], NT) for n in (0, 1)], axis=1
    )
    dq = scale * grown * (mm(kd, dots, NT) + from_state)
    dk = scale * shrunk * mm(qd, dots)
    dv = scale * mm(scores, mix_half, TN)
    state_end = [last[n] * state_ref[n] + mm(ke[:, spans[n]], values[spans[n]]) for n in (0, 1)]
    gq_ref[...] = dq.astype(BF)

    mate = lax.rem(sp, 2) == core

    @pl.when(mate)
    def _():
        waited(all_in.at[pl.ds(0, groups - 1)], pj_r)
        to_tp(all_in, all_in, mate_s, mate_r, z, other)

    after[...] = jnp.zeros_like(after)
    for s in range(1, groups):
        @pl.when(s > sp)
        def _():
            waited(carry_in.at[s], carry_r.at[s])
            after[...] += carry_in[s].astype(F32)

    end_1 = after[...]
    g_end = [local[1] + last[1] * end_1, end_1]
    half_end = [g.astype(BF) for g in g_end]
    dk = dk + to_end * jnp.concatenate(
        [mm(half_end[n], values[spans[n]], NT) for n in (0, 1)], axis=1
    )
    dv = dv + jnp.concatenate([mm(ke[:, spans[n]], half_end[n], TN) for n in (0, 1)], axis=0)
    tails = [jnp.sum(state_end[n] * g_end[n], axis=1, keepdims=True) for n in (0, 1)]
    tail = jnp.concatenate([jnp.broadcast_to(t, (DK, SPAN)) for t in tails], axis=1)
    gd_ref[...] = mm(queries * dq - keys * dk, since, NN, HIGH) + tail
    gk_ref[...] = dk.astype(BF)
    gv_ref[...] = dv.astype(BF)

    @pl.when(jnp.logical_not(mate))
    def _():
        waited(all_in, mate_r)

    waited(all_saved.at[pl.ds(0, groups - 1)], save_r)
    depth = groups * tokens
    gproj_ref[...] = mm(
        all_in[...].reshape(depth, LANE), all_saved[...].reshape(depth, LANE), TN
    )
    drain(6)


def store_kernel(*refs):
    count = (len(refs) - 1) // 2
    sems = refs[-1]
    copies = []
    for n, (src, dst) in enumerate(zip(refs[:count], refs[count : 2 * count])):
        copy = pltpu.make_async_copy(src, dst.at[0] if len(dst.shape) > 2 else dst, sems.at[n])
        copy.start()
        copies.append(copy)
    for copy in copies:
        copy.wait()


def on_device(
    moe_input, cotangent, route_expert, route_weight, w_gate, w_up, w_down, out_proj, saved_out,
    queries, keys, values, log_decay, span_state,
):
    groups, lanes = lax.axis_size("sp"), lax.axis_size("tp")
    tokens, width = moe_input.shape
    capacity = 4 * tokens // groups
    slots = groups * capacity
    hidden = w_gate.shape[2]
    chips = lanes // 2
    firsts = 6
    vmem = pl.BlockSpec(memory_space=pltpu.VMEM)
    hbm = pl.BlockSpec(memory_space=pltpu.HBM)
    dma = pltpu.SemaphoreType.DMA
    shape = jax.ShapeDtypeStruct
    slab = (2, groups, capacity, LANE)
    scratch = [
        pltpu.VMEM((2, tokens), jnp.int32),
        pltpu.VMEM((2, tokens), F32),
        pltpu.VMEM((tokens, width), BF),
        pltpu.VMEM((tokens, width), BF),
        pltpu.VMEM((LANE, width), BF),
        pltpu.VMEM((tokens, LANE), BF),
        pltpu.VMEM((DK, tokens), BF),
        pltpu.VMEM((DK, tokens), BF),
        pltpu.VMEM((tokens, LANE), BF),
        pltpu.VMEM((DK, tokens), F32),
        pltpu.VMEM((2, DK, LANE), F32),
        pltpu.VMEM((width, 2 * hidden), BF),
        pltpu.VMEM((hidden, width), BF),
        pltpu.VMEM((lanes, *slab), BF),
        pltpu.VMEM((hidden, slots), BF),
        pltpu.VMEM((slots, 2 * hidden), BF),
        pltpu.VMEM((slots, 2 * tokens), BF),
        pltpu.VMEM((tokens, slots), BF),
        pltpu.VMEM((firsts, *slab), BF),
        pltpu.VMEM((slots, 2 * hidden), F32),
        pltpu.VMEM((slots, hidden), F32),
        pltpu.VMEM((slots, 2 * LANE), F32),
        pltpu.VMEM((chips, slots, LANE), F32),
        pltpu.VMEM((chips, slots, LANE), BF),
        pltpu.VMEM((chips, slots, LANE), BF),
        pltpu.VMEM((2, slots, LANE), BF),
        pltpu.VMEM((2, slots, LANE), BF),
        pltpu.VMEM((chips, groups, capacity, LANE), BF),
        pltpu.VMEM((chips, groups, capacity, LANE), BF),
        pltpu.VMEM((chips, tokens, LANE), BF),
        pltpu.VMEM((chips, tokens, LANE), BF),
        pltpu.VMEM((lanes, tokens, LANE), BF),
        pltpu.VMEM((groups, tokens, LANE), BF),
        pltpu.VMEM((groups, tokens, LANE), BF),
        pltpu.VMEM((8, LANE), F32),
        pltpu.VMEM((groups, 8, LANE), F32),
        pltpu.VMEM((groups, DK, LANE), BF),
        pltpu.VMEM((groups, DK, LANE), BF),
        pltpu.VMEM((DK, LANE), F32),
        dma((3,)), dma((11,)),
        dma((firsts, 2)), dma((firsts, 2)),
        dma((2, 2, 2)), dma((2, 2, 2)),
        dma((chips,)), dma((chips,)),
        dma((2, 2)), dma((2, 2)),
        dma((chips,)), dma((chips,)),
        dma((2,)), dma((2,)),
        dma((chips,)), dma((chips,)),
        dma((chips,)), dma((chips,)),
        dma((chips,)), dma((chips,)),
        dma((chips,)), dma((chips,)),
        dma, dma, dma((2,)), dma((2,)), dma, dma,
        dma, dma, dma, dma,
        dma((groups,)), dma((groups,)),
    ]
    made = (
        pltpu.VMEM((width, hidden), BF),
        pltpu.VMEM((width, hidden), BF),
        pltpu.VMEM((hidden, width), BF),
        pltpu.VMEM((LANE, LANE), F32),
        pltpu.VMEM((DK, tokens), BF),
        pltpu.VMEM((DK, tokens), BF),
        pltpu.VMEM((tokens, LANE), BF),
        pltpu.VMEM((DK, tokens), F32),
    )
    results = pl.pallas_call(
        functools.partial(main_kernel, groups=groups, lanes=lanes, capacity=capacity),
        name="experts_and_attention",
        out_shape=made,
        in_specs=[hbm] * 14,
        out_specs=(vmem,) * 8,
        scratch_shapes=scratch,
        compiler_params=pltpu.CompilerParams(
            collective_id=0, has_side_effects=True, vmem_limit_bytes=62105600
        ),
    )(
        route_expert.T, route_weight.T, moe_input, cotangent, out_proj, saved_out, queries.T,
        keys.T, values, log_decay.T, span_state, w_gate, w_up, w_down,
    )
    results = pl.pallas_call(
        store_kernel,
        name="store_results",
        out_shape=tuple(
            shape((1, *a.shape) if n < 3 else a.shape, a.dtype) for n, a in enumerate(results)
        ),
        in_specs=[vmem] * 8,
        out_specs=(hbm,) * 8,
        scratch_shapes=[dma((8,))],
        compiler_params=pltpu.CompilerParams(vmem_limit_bytes=1024 * 1024),
    )(*(pltpu.with_memory_space_constraint(r, pltpu.VMEM) for r in results))
    gg, gu, gw, gp, gq, gk, gv, gd = results
    return gg, gu, gw, gp, gq.T, gk.T, gv, gd.T


def solution(mesh):
    placed = (
        P("sp", None),
        P("sp", None),
        P("sp", None),
        P("sp", None),
        P("sp", None, "tp"),
        P("sp", None, "tp"),
        P("sp", "tp", None),
        P("tp", None),
        P("sp", "tp"),
        P("sp", "tp"),
        P("sp", "tp"),
        P("sp", "tp"),
        P("sp", "tp"),
        P("sp", "tp", None),
    )
    return jax.shard_map(
        on_device,
        mesh=mesh,
        in_specs=placed,
        out_specs=(
            P("sp", None, "tp"),
            P("sp", None, "tp"),
            P("sp", "tp", None),
            P("sp", "tp"),
            P("sp", "tp"),
            P("sp", "tp"),
            P("sp", "tp"),
            P("sp", "tp"),
        ),
        check_vma=False,
    )
```

```python
import functools

import jax
import jax.numpy as jnp
from jax import lax
from jax.experimental import pallas as pl
from jax.experimental.pallas import tpu as pltpu
from jax.sharding import PartitionSpec as P

BF = jnp.bfloat16
F32 = jnp.float32
HIGH = lax.Precision.HIGHEST
LANE = 128
DK = 64
SPAN = 64
NN = (((1,), (0,)), ((), ()))
NT = (((1,), (1,)), ((), ()))
TN = (((0,), (0,)), ((), ()))


def mm(a, b, dims=NN, precision=None):
    return lax.dot_general(a, b, dims, precision=precision, preferred_element_type=F32)


def half_dot(a, b, dims=NN):
    return mm(a.astype(BF), b.astype(BF), dims)


def waited(ref, sem):
    pltpu.make_async_copy(ref, ref, sem).wait()


def main_kernel(
    route_hbm, weight_hbm, input_hbm, cot_hbm, proj_hbm, saved_hbm, q_hbm, k_hbm, v_hbm, log_hbm,
    state_hbm, wg_hbm, wu_hbm, wd_hbm,
    gg_ref, gu_ref, gw_ref, gproj_ref, gq_ref, gk_ref, gv_ref, gd_ref,
    route_ref, weight_ref, input_ref, cot_ref, proj_ref, saved_ref, q_ref, k_ref, v_ref, log_ref,
    state_ref, wgu, wd, rows, hid_t, dgu, table, picks, send, gu_acc, hid_acc, tmp, mine, pair_out,
    pair_in, near_out, near_in, back_out, back_in, far_out, far_in, grad_in, all_in, all_saved,
    tot_out, tot_in,
    carry_out, carry_in, after,
    w_sem, load_sem, disp_s, disp_r, ring_s, ring_r, core_s, core_r, late_s, late_r, pair_s, pair_r, near_s, near_r, back_s, back_r,
    far_s, far_r, all_s, all_r, fwd_s, fwd_r, save_s, save_r, opp_s, opp_r, mate_s, mate_r, pj_s, pj_r, tot_s, tot_r, carry_s, carry_r,
    *, groups, lanes, capacity,
):
    chips = lanes // 2
    sp, tp = lax.axis_index("sp"), lax.axis_index("tp")
    z, core = lax.div(tp, 2), lax.rem(tp, 2)
    other = 1 - core
    tokens = input_ref.shape[0]
    slots = groups * capacity
    hidden = wd.shape[0]

    def wrapped(rel):
        return lax.rem(z + rel, chips)

    def to(src, dst, send_sem, recv_sem, **where):
        pltpu.make_async_remote_copy(
            src_ref=src, dst_ref=dst, send_sem=send_sem, recv_sem=recv_sem,
            device_id=where, device_id_type=pl.DeviceIdType.MESH,
        ).start()

    def to_tp(src, dst, send_sem, recv_sem, chip, at_core):
        to(src, dst, send_sem, recv_sem, tp=chip * 2 + at_core)

    barrier = pltpu.get_barrier_semaphore()

    @pl.loop(1, groups)
    def _(o):
        pl.semaphore_signal(
            barrier, inc=1, device_id={"sp": lax.rem(sp + o, groups)},
            device_id_type=pl.DeviceIdType.MESH,
        )

    @pl.loop(1, chips)
    def _(o):
        pl.semaphore_signal(
            barrier, inc=1, device_id={"tp": wrapped(o) * 2 + core},
            device_id_type=pl.DeviceIdType.MESH,
        )

    pl.semaphore_signal(
        barrier, inc=1, device_id={"tp": z * 2 + other}, device_id_type=pl.DeviceIdType.MESH
    )

    given = [
        route_hbm, weight_hbm, input_hbm, cot_hbm, log_hbm, proj_hbm, saved_hbm, q_hbm, k_hbm,
        v_hbm, state_hbm,
    ]
    held = [
        route_ref, weight_ref, input_ref, cot_ref, log_ref, proj_ref, saved_ref, q_ref, k_ref,
        v_ref, state_ref,
    ]
    loads = [
        pltpu.make_async_copy(src, dst, load_sem.at[n])
        for n, (src, dst) in enumerate(zip(given, held))
    ]
    for copy in loads[:5]:
        copy.start()
    copies = [
        pltpu.make_async_copy(wg_hbm.at[0], wgu.at[:, pl.ds(0, hidden)], w_sem.at[0]),
        pltpu.make_async_copy(wu_hbm.at[0], wgu.at[:, pl.ds(hidden, hidden)], w_sem.at[1]),
        pltpu.make_async_copy(wd_hbm.at[0], wd, w_sem.at[2]),
    ]
    for copy in loads[:2]:
        copy.wait()
    experts = lax.broadcasted_iota(jnp.int32, (groups, tokens), 0)
    named = [(route_ref[j : j + 1, :] == experts).astype(F32) for j in (0, 1)]
    row = lax.broadcasted_iota(jnp.int32, (tokens, tokens), 0)
    col = lax.broadcasted_iota(jnp.int32, (tokens, tokens), 1)
    earlier = half_dot(named[0] + named[1], (row < col).astype(F32))
    place_in = lax.broadcasted_iota(jnp.int32, (slots, tokens), 0)
    found = []
    for j in (0, 1):
        place = jnp.sum(earlier * named[j], axis=0, keepdims=True).astype(jnp.int32)
        slot = route_ref[j : j + 1, :] * capacity + place
        found.append((slot == place_in).astype(F32))
        table[:, j * tokens : (j + 1) * tokens] = found[j].astype(BF)
    picks[...] = jnp.transpose(found[0] + found[1]).astype(BF)
    weights = jnp.transpose(
        jnp.concatenate([weight_ref[...], jnp.zeros((6, tokens), F32)], axis=0)
    )
    far_blocks = range(3, chips - 2)
    late = (2, chips - 2)
    firsts = [0, *far_blocks, *late]

    def fill(b, rel):
        t = wrapped(rel) * 2 + core
        columns = pl.ds(pl.multiple_of(t * LANE, LANE), LANE)
        if rel not in late:
            ours = input_ref[:, columns]
            ins = mm(table[...], jnp.concatenate([ours, ours], axis=0))
            send[b, 0] = ins.astype(BF).reshape(groups, capacity, LANE)
            rows[t, 0, sp] = send[b, 0, sp]
        cot = cot_ref[:, columns].astype(F32)
        weighted = [(weights[:, j : j + 1] * cot).astype(BF) for j in (0, 1)]
        cots = mm(table[...], jnp.concatenate(weighted, axis=0))
        send[b, 1] = cots.astype(BF).reshape(groups, capacity, LANE)
        rows[t, 1, sp] = send[b, 1, sp]

    def dispatch(b, rel, p):
        t = wrapped(rel) * 2 + core

        @pl.loop(1, groups)
        def _(o):
            peer = lax.rem(sp + o, groups)
            to(send.at[b, p, peer], rows.at[t, p, sp], disp_s.at[b, p], disp_r.at[b, p], sp=peer)

    def pieces(rel):
        return (1,) if rel in late else (0, 1)

    for copy in loads[2:5]:
        copy.wait()
    for copy in [*loads[5:], *copies]:
        copy.start()
    fill(0, 0)
    totals = mm(jnp.ones((8, tokens), F32), log_ref[...], NT, HIGH)
    tot_out[...] = jnp.concatenate(
        [totals, jnp.zeros((8, LANE - DK), F32)], axis=1
    )
    tot_in[sp] = tot_out[...]
    pl.semaphore_wait(barrier, groups - 1 + chips)

    for b, rel in enumerate(firsts):
        if b:
            fill(b, rel)
        for p in pieces(rel):
            dispatch(b, rel, p)

    @pl.loop(1, groups)
    def _(o):
        peer = lax.rem(sp + o, groups)
        to(tot_out, tot_in.at[sp], tot_s, tot_r, sp=peer)

    for copy in loads[5:]:
        copy.wait()
    gu_acc[...] = jnp.zeros_like(gu_acc)
    hid_acc[...] = jnp.zeros_like(hid_acc)

    def block(rel):
        return wrapped(rel) * 2 + core

    def pass_ring(rel, step, p, side):
        chip = wrapped(1 if side == 0 else chips - 1)
        part = rows.at[block(rel), p]
        to_tp(part, part, ring_s.at[step, side, p], ring_r.at[step, side, p], chip, core)

    def await_ring(rel, step, p, side):
        waited(rows.at[block(rel), p], ring_r.at[step, side, p])

    def to_other(rel):
        t = block(rel)
        to_tp(rows.at[t], rows.at[t], core_s.at[rel], core_r.at[rel], z, other)

    def from_other(rel):
        waited(rows.at[wrapped(rel) * 2 + other], core_r.at[rel])

    def late_to_other(i, p):
        part = rows.at[block(late[i]), p]
        to_tp(part, part, late_s.at[i, p], late_r.at[i, p], z, other)

    def both(zz, p):
        return jnp.concatenate(
            [rows[zz * 2 + k, p].reshape(slots, LANE) for k in (0, 1)], axis=1
        )

    def depth_of(zz):
        return pl.ds(pl.multiple_of(zz * 2 * LANE, 2 * LANE), 2 * LANE)

    def gather_product(rel):
        zz = wrapped(rel)
        gu_acc[...] += mm(both(zz, 0), wgu[depth_of(zz), :])
        hid_acc[...] += mm(both(zz, 1), wd[:, depth_of(zz)], NT)

    def await_dispatch(b, p):
        waited(send.at[b, p, pl.ds(0, groups - 1)], disp_r.at[b, p])

    def drain(phase):
        if phase >= 2:
            for b, rel in enumerate(firsts):
                for p in pieces(rel):
                    waited(send.at[b, p, pl.ds(0, groups - 1)], disp_s.at[b, p])
            waited(tot_in.at[pl.ds(0, groups - 1)], tot_s)
        if phase >= 3:
            for side in (0, 1):
                waited(rows.at[0, 0], ring_s.at[0, side, 0])
                waited(rows.at[0, 0], ring_s.at[0, side, 1])
                waited(rows.at[0, 0], ring_s.at[1, side, 0])
                for p in (0, 1):
                    waited(rows.at[0, 0], late_s.at[side, p])
            for rel in range(chips):
                if rel not in late:
                    waited(rows.at[0], core_s.at[rel])
        if phase >= 4:
            waited(all_saved.at[pl.ds(0, groups - 1)], save_s)
            for j in range(chips):
                waited(pair_out.at[j], pair_s.at[j])
                if j in (2, 3):
                    waited(near_out.at[j - 2], near_s.at[j - 2])
                else:
                    waited(back_out.at[j, pl.ds(0, groups - 1)], back_s.at[j])
                    if j < chips - 1:
                        waited(far_out.at[j], far_s.at[j])
        if phase >= 5:
            for rel in range(chips):
                waited(grad_in.at[0], fwd_s.at[rel])
                if rel not in (0, chips // 2):
                    waited(grad_in.at[0], all_s.at[rel])
            for side in (0, 1):
                waited(grad_in.at[0, pl.ds(0, tokens // 2)], opp_s.at[side])
        if phase >= 6:
            @pl.when(lax.rem(sp, 2) == core)
            def _():
                waited(all_in.at[pl.ds(0, chips - 1)], pj_s)
                waited(all_in, mate_s)

            @pl.when(lax.rem(sp, 2) != core)
            def _():
                waited(all_in.at[pl.ds(0, chips)], pj_s)

            for r in range(groups - 1):
                @pl.when(sp > r)
                def _():
                    waited(carry_out.at[r], carry_s.at[r])

    for p in (0, 1):
        await_dispatch(0, p)
        for side in (0, 1):
            pass_ring(0, 0, p, side)
    to_other(0)
    for copy in copies:
        copy.wait()
    from_other(0)
    gather_product(0)
    for side in (0, 1):
        rel = chips - 1 if side == 0 else 1
        await_ring(rel, 0, 0, side)
        pass_ring(rel, 1, 0, side)
    for p in (0, 1):
        await_dispatch(1, p)
    to_other(firsts[1])
    for side in (0, 1):
        rel = chips - 1 if side == 0 else 1
        await_ring(rel, 0, 1, side)
        to_other(rel)
    for p in (0, 1):
        await_dispatch(2, p)
    to_other(firsts[2])

    @pl.loop(0, 2)
    def _(i):
        rel = 1 + i * (chips - 2)
        from_other(rel)
        gather_product(rel)

    for p in (0, 1):
        await_dispatch(3, p)
    to_other(firsts[3])

    @pl.loop(0, len(far_blocks) - 1)
    def _(i):
        rel = far_blocks[0] + i
        from_other(rel)
        gather_product(rel)

    for i in (0, 1):
        await_ring(late[i], 1, 0, 1 - i)
        late_to_other(i, 0)
    from_other(far_blocks[-1])
    gather_product(far_blocks[-1])
    for i in (0, 1):
        await_dispatch(4 + i, 1)
        late_to_other(i, 1)
    for p in (0, 1):
        for i in (0, 1):
            zz = wrapped(late[i])
            waited(rows.at[zz * 2 + other, p], late_r.at[i, p])
            if p == 0:
                gu_acc[...] += mm(both(zz, 0), wgu[depth_of(zz), :])
            else:
                hid_acc[...] += mm(both(zz, 1), wd[:, depth_of(zz)], NT)

    tile = LANE

    @pl.loop(0, slots // tile)
    def _(i):
        at = pl.ds(pl.multiple_of(i * tile, tile), tile)
        gate = gu_acc[at, :hidden]
        upper = gu_acc[at, hidden:]
        d_hidden = hid_acc[at, :]
        sigmoid = jax.nn.sigmoid(gate)
        active = gate * sigmoid
        hid_t[:, at] = jnp.transpose(active * upper).astype(BF)
        dgu[at, hidden:] = (d_hidden * active).astype(BF)
        dgu[at, :hidden] = (
            d_hidden * upper * sigmoid * (1.0 + gate * (1.0 - sigmoid))
        ).astype(BF)

    def turn(j):
        k = jnp.where(j < 2, j, j - 2)
        far = chips // 2 + lax.div(k + 1, 2) * (2 * lax.rem(k, 2) - 1)
        near = 1 + (j - 2) * (chips - 2)
        return jnp.where((j == 2) | (j == 3), near, jnp.where(j == chips - 1, 0, far))

    def slot_block(j):
        zz = wrapped(turn(j))
        depth = pl.ds(pl.multiple_of(zz * 2 * LANE, 2 * LANE), 2 * LANE)
        tmp[...] = mm(dgu[...], wgu[depth, :], NT)
        pair_out[j] = tmp[:, pl.ds(pl.multiple_of(other * LANE, LANE), LANE)].astype(BF)
        mine[j] = tmp[:, pl.ds(pl.multiple_of(core * LANE, LANE), LANE)]
        to_tp(pair_out.at[j], pair_in.at[j], pair_s.at[j], pair_r.at[j], z, other)

    def slot_near(j):
        waited(pair_in.at[j], pair_r.at[j])
        side = j - 2
        near_out[side] = (mine[j] + pair_in[j].astype(F32)).astype(BF)
        to_tp(
            near_out.at[side], near_in.at[side], near_s.at[side], near_r.at[side],
            wrapped(turn(j)), core,
        )

    def slot_send(j, whole):
        back_out[j] = whole.astype(BF).reshape(groups, capacity, LANE)
        back_in[j, sp] = back_out[j, sp]

        @pl.loop(1, groups)
        def _(o):
            peer = lax.rem(sp + o, groups)
            to(back_out.at[j, peer], back_in.at[j, sp], back_s.at[j], back_r.at[j], sp=peer)

    def slot_return(j):
        waited(pair_in.at[j], pair_r.at[j])
        slot_send(j, mine[j] + pair_in[j].astype(F32))

    lag = 2

    @pl.loop(0, chips + lag - 1)
    def _(j):
        @pl.when(j < chips)
        def _():
            slot_block(j)

        i = j - lag

        @pl.when((i == 2) | (i == 3))
        def _():
            slot_near(i)

        @pl.when((i >= 0) & (i != 2) & (i != 3))
        def _():
            slot_return(i)

    def weight_block(zz):
        depth = depth_of(zz)
        pair = mm(both(zz, 0), dgu[...], TN).astype(BF)
        gg_ref[depth, :] = pair[:, :hidden]
        gu_ref[depth, :] = pair[:, hidden:]
        gw_ref[:, depth] = mm(hid_t[...], both(zz, 1)).astype(BF)

    weight_block(0)
    weight_block(1)
    own = chips - 1
    waited(pair_in.at[own], pair_r.at[own])
    summed = mine[own] + pair_in[own].astype(F32)
    for j in (0, 1):
        waited(near_in.at[j], near_r.at[j])
        summed += near_in[j].astype(F32)
    slot_send(own, summed)

    @pl.loop(1, groups)
    def _(o):
        peer = lax.rem(sp + o, groups)
        to(saved_ref, all_saved.at[sp], save_s, save_r, sp=peer)

    all_saved[sp] = saved_ref[...]

    def routed(j):
        waited(back_out.at[j, pl.ds(0, groups - 1)], back_r.at[j])
        return mm(picks[...], back_in[j].reshape(slots, LANE))

    @pl.loop(0, chips - 3)
    def _(i):
        j = jnp.where(i < 2, i, i + 2)
        rel = turn(j)
        far_out[j] = routed(j).astype(BF)
        to_tp(far_out.at[j], far_in.at[rel], far_s.at[j], far_r.at[rel], wrapped(rel), core)
        weight_block(i + 2)

    weight_block(chips - 1)
    total = routed(chips - 1)
    same_span = lax.div(row, SPAN) == lax.div(col, SPAN)
    causal = (row >= col) & same_span
    until = ((row <= col) & same_span).astype(F32)
    since = causal.astype(F32)
    cum = mm(log_ref[...], until, NN, HIGH)
    waited(tot_in.at[pl.ds(0, groups - 1)], tot_r)
    after_row = lax.broadcasted_iota(jnp.int32, (groups, LANE), 0)
    after_col = lax.broadcasted_iota(jnp.int32, (groups, LANE), 1)
    between = ((after_row > after_col) & (after_row < sp)).astype(F32)
    factors = jnp.exp(mm(tot_in[:, 0, :DK], between, TN, HIGH))

    for rel in range(2, chips - 1):
        waited(far_in.at[rel], far_r.at[rel])
        total += far_in[rel].astype(F32)
    columns = pl.ds(pl.multiple_of(tp * LANE, LANE), LANE)
    grad_in[tp] = (cot_ref[:, columns].astype(F32) + total).astype(BF)
    reach = chips // 2 - 1
    order = [r for k in range(reach, 0, -1) for r in (k, chips - k)]
    for rel in order:
        to_tp(grad_in.at[tp], grad_in.at[tp], all_s.at[rel], all_r.at[rel], wrapped(rel), core)
    to_tp(grad_in.at[tp], grad_in.at[tp], fwd_s.at[0], fwd_r.at[0], z, other)

    def to_owner(t):
        @pl.when(t != sp)
        def _():
            to(grad_in.at[t], all_in.at[sp], pj_s, pj_r, sp=t)

        @pl.when(t == sp)
        def _():
            all_in[sp] = grad_in[t]

    def to_pair(rel, t):
        to_tp(grad_in.at[t], grad_in.at[t], fwd_s.at[rel], fwd_r.at[rel], z, other)

    half_rows = tokens // 2
    to_owner(tp)
    for rel in order:
        t = wrapped(chips - rel) * 2 + core
        waited(grad_in.at[t], all_r.at[rel])
        if rel in (reach, chips - reach):
            side = 0 if rel == reach else 1
            part = grad_in.at[t, pl.ds(side * half_rows, half_rows)]
            chip = wrapped(1 if side == 0 else chips - 1)
            to_tp(part, part, opp_s.at[side], opp_r.at[side], chip, core)
        to_pair(rel, t)
        to_owner(t)
    t = wrapped(chips // 2) * 2 + core
    for side in (0, 1):
        waited(grad_in.at[t, pl.ds(0, half_rows)], opp_r.at[side])
    to_pair(chips // 2, t)
    to_owner(t)
    mix = jnp.zeros((tokens, LANE), F32)
    for rel in [0, *order, chips // 2]:
        zz = wrapped(chips - rel if rel else 0)
        waited(grad_in.at[zz * 2 + other], fwd_r.at[rel])
        pair = jnp.concatenate([grad_in[2 * zz], grad_in[2 * zz + 1]], axis=1)
        mix += mm(pair, proj_ref[:, depth_of(zz)], NT)

    scale = DK ** (-0.5)
    grown = jnp.exp(cum)
    shrunk = jnp.exp(-cum)
    queries = q_ref[...].astype(F32)
    keys = k_ref[...].astype(F32)
    qd = (queries * grown).astype(BF)
    kd = (keys * shrunk).astype(BF)
    mix_half = mix.astype(BF)
    spans = [slice(n * SPAN, (n + 1) * SPAN) for n in (0, 1)]
    local = [scale * mm(qd[:, s], mix_half[s]) for s in spans]
    ends = [cum[:, (n + 1) * SPAN - 1 : (n + 1) * SPAN] for n in (0, 1)]
    last = [jnp.exp(e) for e in ends]
    begin = local[0] + last[0] * local[1]
    for r in range(groups - 1):
        @pl.when(sp > r)
        def _():
            carry_out[r] = (begin * factors[:, r : r + 1]).astype(BF)
            to(carry_out.at[r], carry_in.at[sp], carry_s.at[r], carry_r.at[sp], sp=r)

    values = v_ref[...]
    to_end = jnp.concatenate([jnp.exp(ends[n] - cum[:, spans[n]]) for n in (0, 1)], axis=1)
    ke = (keys * to_end).astype(BF)
    scores = jnp.where(causal, mm(qd, kd, TN), 0.0).astype(BF)
    dots = jnp.where(causal, mm(mix_half, values, NT), 0.0).astype(BF)
    from_state = jnp.concatenate(
        [mm(state_ref[n].astype(BF), mix_half[spans[n]], NT) for n in (0, 1)], axis=1
    )
    dq = scale * grown * (mm(kd, dots, NT) + from_state)
    dk = scale * shrunk * mm(qd, dots)
    dv = scale * mm(scores, mix_half, TN)
    state_end = [last[n] * state_ref[n] + mm(ke[:, spans[n]], values[spans[n]]) for n in (0, 1)]
    gq_ref[...] = dq.astype(BF)

    mate = lax.rem(sp, 2) == core

    @pl.when(mate)
    def _():
        waited(all_in.at[pl.ds(0, groups - 1)], pj_r)
        to_tp(all_in, all_in, mate_s, mate_r, z, other)

    @pl.when(jnp.logical_not(mate))
    def _():
        waited(all_in, mate_r)

    waited(all_saved.at[pl.ds(0, groups - 1)], save_r)
    depth = groups * tokens
    gproj_ref[...] = mm(
        all_in[...].reshape(depth, LANE), all_saved[...].reshape(depth, LANE), TN
    )

    after[...] = jnp.zeros_like(after)
    for s in range(1, groups):
        @pl.when(s > sp)
        def _():
            waited(carry_in.at[s], carry_r.at[s])
            after[...] += carry_in[s].astype(F32)

    end_1 = after[...]
    g_end = [local[1] + last[1] * end_1, end_1]
    half_end = [g.astype(BF) for g in g_end]
    dk = dk + to_end * jnp.concatenate(
        [mm(half_end[n], values[spans[n]], NT) for n in (0, 1)], axis=1
    )
    dv = dv + jnp.concatenate([mm(ke[:, spans[n]], half_end[n], TN) for n in (0, 1)], axis=0)
    tails = [jnp.sum(state_end[n] * g_end[n], axis=1, keepdims=True) for n in (0, 1)]
    tail = jnp.concatenate([jnp.broadcast_to(t, (DK, SPAN)) for t in tails], axis=1)
    gd_ref[...] = mm(queries * dq - keys * dk, since, NN, HIGH) + tail
    gk_ref[...] = dk.astype(BF)
    gv_ref[...] = dv.astype(BF)

    drain(6)


def store_kernel(*refs):
    count = (len(refs) - 1) // 2
    sems = refs[-1]
    copies = []
    for src, dst in zip(refs[:count], refs[count : 2 * count]):
        if len(dst.shape) > 2:
            rows = src.shape[0] // 4
            pairs = [
                (src.at[pl.ds(k * rows, rows)], dst.at[0, pl.ds(k * rows, rows)]) for k in range(4)
            ]
        else:
            pairs = [(src, dst)]
        for part, place in pairs:
            copies.append(pltpu.make_async_copy(part, place, sems.at[len(copies)]))
    for copy in copies:
        copy.start()
    for copy in copies:
        copy.wait()


def on_device(
    moe_input, cotangent, route_expert, route_weight, w_gate, w_up, w_down, out_proj, saved_out,
    queries, keys, values, log_decay, span_state,
):
    groups, lanes = lax.axis_size("sp"), lax.axis_size("tp")
    tokens, width = moe_input.shape
    capacity = 4 * tokens // groups
    slots = groups * capacity
    hidden = w_gate.shape[2]
    chips = lanes // 2
    firsts = 6
    vmem = pl.BlockSpec(memory_space=pltpu.VMEM)
    hbm = pl.BlockSpec(memory_space=pltpu.HBM)
    dma = pltpu.SemaphoreType.DMA
    shape = jax.ShapeDtypeStruct
    slab = (2, groups, capacity, LANE)
    scratch = [
        pltpu.VMEM((2, tokens), jnp.int32),
        pltpu.VMEM((2, tokens), F32),
        pltpu.VMEM((tokens, width), BF),
        pltpu.VMEM((tokens, width), BF),
        pltpu.VMEM((LANE, width), BF),
        pltpu.VMEM((tokens, LANE), BF),
        pltpu.VMEM((DK, tokens), BF),
        pltpu.VMEM((DK, tokens), BF),
        pltpu.VMEM((tokens, LANE), BF),
        pltpu.VMEM((DK, tokens), F32),
        pltpu.VMEM((2, DK, LANE), F32),
        pltpu.VMEM((width, 2 * hidden), BF),
        pltpu.VMEM((hidden, width), BF),
        pltpu.VMEM((lanes, *slab), BF),
        pltpu.VMEM((hidden, slots), BF),
        pltpu.VMEM((slots, 2 * hidden), BF),
        pltpu.VMEM((slots, 2 * tokens), BF),
        pltpu.VMEM((tokens, slots), BF),
        pltpu.VMEM((firsts, *slab), BF),
        pltpu.VMEM((slots, 2 * hidden), F32),
        pltpu.VMEM((slots, hidden), F32),
        pltpu.VMEM((slots, 2 * LANE), F32),
        pltpu.VMEM((chips, slots, LANE), F32),
        pltpu.VMEM((chips, slots, LANE), BF),
        pltpu.VMEM((chips, slots, LANE), BF),
        pltpu.VMEM((2, slots, LANE), BF),
        pltpu.VMEM((2, slots, LANE), BF),
        pltpu.VMEM((chips, groups, capacity, LANE), BF),
        pltpu.VMEM((chips, groups, capacity, LANE), BF),
        pltpu.VMEM((chips, tokens, LANE), BF),
        pltpu.VMEM((chips, tokens, LANE), BF),
        pltpu.VMEM((lanes, tokens, LANE), BF),
        pltpu.VMEM((groups, tokens, LANE), BF),
        pltpu.VMEM((groups, tokens, LANE), BF),
        pltpu.VMEM((8, LANE), F32),
        pltpu.VMEM((groups, 8, LANE), F32),
        pltpu.VMEM((groups, DK, LANE), BF),
        pltpu.VMEM((groups, DK, LANE), BF),
        pltpu.VMEM((DK, LANE), F32),
        dma((3,)), dma((11,)),
        dma((firsts, 2)), dma((firsts, 2)),
        dma((2, 2, 2)), dma((2, 2, 2)),
        dma((chips,)), dma((chips,)),
        dma((2, 2)), dma((2, 2)),
        dma((chips,)), dma((chips,)),
        dma((2,)), dma((2,)),
        dma((chips,)), dma((chips,)),
        dma((chips,)), dma((chips,)),
        dma((chips,)), dma((chips,)),
        dma((chips,)), dma((chips,)),
        dma, dma, dma((2,)), dma((2,)), dma, dma,
        dma, dma, dma, dma,
        dma((groups,)), dma((groups,)),
    ]
    made = (
        pltpu.VMEM((width, hidden), BF),
        pltpu.VMEM((width, hidden), BF),
        pltpu.VMEM((hidden, width), BF),
        pltpu.VMEM((LANE, LANE), F32),
        pltpu.VMEM((DK, tokens), BF),
        pltpu.VMEM((DK, tokens), BF),
        pltpu.VMEM((tokens, LANE), BF),
        pltpu.VMEM((DK, tokens), F32),
    )
    results = pl.pallas_call(
        functools.partial(main_kernel, groups=groups, lanes=lanes, capacity=capacity),
        name="experts_and_attention",
        out_shape=made,
        in_specs=[hbm] * 14,
        out_specs=(vmem,) * 8,
        scratch_shapes=scratch,
        compiler_params=pltpu.CompilerParams(
            collective_id=0, has_side_effects=True, vmem_limit_bytes=62105600
        ),
    )(
        route_expert.T, route_weight.T, moe_input, cotangent, out_proj, saved_out, queries.T,
        keys.T, values, log_decay.T, span_state, w_gate, w_up, w_down,
    )
    results = pl.pallas_call(
        store_kernel,
        name="store_results",
        out_shape=tuple(
            shape((1, *a.shape) if n < 3 else a.shape, a.dtype) for n, a in enumerate(results)
        ),
        in_specs=[vmem] * 8,
        out_specs=(hbm,) * 8,
        scratch_shapes=[dma((17,))],
        compiler_params=pltpu.CompilerParams(vmem_limit_bytes=1024 * 1024),
    )(*(pltpu.with_memory_space_constraint(r, pltpu.VMEM) for r in results))
    gg, gu, gw, gp, gq, gk, gv, gd = results
    return gg, gu, gw, gp, gq.T, gk.T, gv, gd.T


def solution(mesh):
    placed = (
        P("sp", None),
        P("sp", None),
        P("sp", None),
        P("sp", None),
        P("sp", None, "tp"),
        P("sp", None, "tp"),
        P("sp", "tp", None),
        P("tp", None),
        P("sp", "tp"),
        P("sp", "tp"),
        P("sp", "tp"),
        P("sp", "tp"),
        P("sp", "tp"),
        P("sp", "tp", None),
    )
    return jax.shard_map(
        on_device,
        mesh=mesh,
        in_specs=placed,
        out_specs=(
            P("sp", None, "tp"),
            P("sp", None, "tp"),
            P("sp", "tp", None),
            P("sp", "tp"),
            P("sp", "tp"),
            P("sp", "tp"),
            P("sp", "tp"),
            P("sp", "tp"),
        ),
        check_vma=False,
    )
```
